256 devices in a mesh: sp: 32 (over z, y), tp: 8 (over x, core).
Axes of the slice: x: 4, y: 4, z: 8, core: 2. Of those that a mesh axis runs over, the one named last changes fastest.
Arguments:
- prompt: bfloat16 [4, 6144, 4096], P(None, 'sp'), may hold values from -6 to 6
- forget_weight: bfloat16 [4096, 2048], P(None, 'tp'), may hold values from -0.09375 to 0.09375
- value_weight: bfloat16 [4096, 2048], P(None, 'tp'), may hold values from -1.5 to 1.5
- lower_bound: float32 [2048], P('tp'), may hold values from 0.9 to 0.99991862
- extra_decay: float32 [4, 6144, 2048], P(None, 'sp', 'tp'), may hold values from -1.40113932 to 0
- new_token: bfloat16 [4, 4096], P(None, 'tp'), may hold values from -6 to 6
- new_query: bfloat16 [4, 2048], P(None, 'tp'), may hold values from -6 to 6
- read_gain: float32 [128], replicated, may hold values from 0.1 to 1.9
Outputs:
- state_cache: bfloat16 [128, 16, 4, 128], P('sp', 'tp')
- first_read: bfloat16 [4, 2048], P(None, 'tp')
The draws below stay inside these ranges and needn't reach their ends.
All inputs are finite; a program needn't handle non-finite values.
Results may differ from the reference program's by a relative error of at most 0.0019.
The reference program's roundings to bfloat16 on the way (of `forget_pre`, `values` and `weighted`) count: a program that leaves them out, or rounds other values in their place, can miss the bound.
Values may be sent and summed in bfloat16 or wider, within the bound.
No kernel may reach another device: no remote copies, remote signals or barrier semaphores. Data moves between devices by JAX's collectives and lax.ppermute only.
A program may use at most 64 MiB of HBM per device.

```python
import math
import jax
import jax.numpy as jnp
from jax import lax

D = 4096
H = 16
HD = 128
PROMPT_COUNT = 4
SPAN = 192
W = 2048
SEQLEN = 6144


def draw_prompt(key, part):
    base_key = jax.random.fold_in(key, 5)
    drawn = jnp.clip(jax.random.normal(base_key, (PROMPT_COUNT, SEQLEN, D), jnp.float32), -6.0, 6.0)
    positions = jnp.arange(SEQLEN, dtype=jnp.int32)
    quiet = jnp.where(positions >= SEQLEN - 3 * SPAN, 0.03, 1.0).astype(jnp.float32)
    return (drawn * quiet[None, :, None]).astype(jnp.bfloat16)


def draw_lower_bound(key, part):
    head_key, slow_key, fast_key = jax.random.split(jax.random.fold_in(key, 11), 3)
    share = 0.5
    fast_heads = jax.random.bernoulli(head_key, share, (H,))
    fast_cols = jnp.repeat(fast_heads, HD)
    slow_value = 1.0 - jax.random.uniform(slow_key, (H * HD,), jnp.float32, 0.5, 1.5) / SEQLEN
    fast_value = jax.random.uniform(fast_key, (H * HD,), jnp.float32, 0.965, 0.98)
    return jnp.where(fast_cols, fast_value, slow_value).astype(jnp.float32)


def draw_extra_decay(key, part):
    decay_rate_key, jitter_random_key, location_random_key, spike_random_key, channel_random_key, mixing_random_key = jax.random.split(jax.random.fold_in(key, 23), 6)
    lower_rate, upper_rate = (0.25, 1.0)
    block_count = SEQLEN // SPAN
    block_rate = jnp.exp(jax.random.uniform(decay_rate_key, (PROMPT_COUNT, block_count, 1, 1), jnp.float32, math.log(lower_rate), math.log(upper_rate)))
    channel_factor = jnp.exp(jax.random.uniform(channel_random_key, (PROMPT_COUNT, 1, 1, W), jnp.float32, -1.0, 1.0))
    block_channel = jnp.exp(jax.random.uniform(mixing_random_key, (PROMPT_COUNT, block_count, 1, W), jnp.float32, -0.5, 0.5))
    roughness = jax.random.uniform(jitter_random_key, (PROMPT_COUNT, block_count, SPAN, W), jnp.float32, 0.5, 1.5)
    chosen_locations = jax.random.randint(location_random_key, (PROMPT_COUNT, 2), 0, SEQLEN)
    spike_length = jax.random.uniform(spike_random_key, (PROMPT_COUNT, 2), jnp.float32, 0.22, 0.69)
    token_positions = jnp.arange(SEQLEN, dtype=jnp.int32)
    spike_events = jnp.sum((token_positions[None, None, :] == chosen_locations[:, :, None]).astype(jnp.float32) * spike_length[:, :, None], axis=1)
    steady_baseline = (block_rate * channel_factor * block_channel * roughness).reshape(PROMPT_COUNT, SEQLEN, W) / SEQLEN
    return (-steady_baseline - spike_events[:, :, None]).astype(jnp.float32)


def block_scale(stream_key, dims, cuts, low, top_value):
    gain, own = 1.0, jax.random.fold_in(stream_key, 6)
    for axis_at, parts in cuts:
        draws = jnp.exp(jax.random.uniform(jax.random.fold_in(own, axis_at), (parts,), jnp.float32, low / len(cuts), top_value / len(cuts)))
        gain = gain * jnp.repeat(draws, dims[axis_at] // parts).reshape([-1 if axis == axis_at else 1 for axis in range(len(dims))])
    return gain


def centred(rng, dims, width, bound, pieces=(), held_as=jnp.bfloat16):
    values = jax.random.normal(rng, dims, jnp.float32) * width
    if len(pieces) > 0:
        values = block_scale(rng, dims, pieces, -0.22, 0.18) * values
    return jnp.clip(values, min=-bound, max=bound).astype(held_as)


def setup_inputs(seed: int = 0) -> dict:
    splits = jax.random.split(jax.random.key(seed), 9)
    return {
        "prompt": draw_prompt(jax.random.fold_in(splits[8], 71), 0),
        "forget_weight": centred(splits[1], (D, W), D ** -0.5, 0.09375, ((1, 8),)),
        "value_weight": centred(splits[2], (D, W), 0.25, 1.5, ((1, 8),)),
        "lower_bound": draw_lower_bound(jax.random.fold_in(splits[8], 71), 0),
        "extra_decay": draw_extra_decay(jax.random.fold_in(splits[8], 71), 0),
        "new_token": centred(splits[5], (PROMPT_COUNT, D), 1.0, 6.0, ((1, 8),)),
        "new_query": centred(splits[6], (PROMPT_COUNT, W), 1.0, 6.0, ((1, 8),)),
        "read_gain": jnp.clip(1.0 + 0.18 * jax.random.normal(splits[7], (HD,), jnp.float32), 0.1, 1.9),
    }


def reference(prompt, forget_weight, value_weight, lower_bound, extra_decay, new_token, new_query, read_gain):
    log_lower = jnp.log(lower_bound)
    log_upper = jnp.log1p(-lower_bound)
    opening = 1.0 - lower_bound
    head_count = W // HD
    block_count = SEQLEN // SPAN

    def one_sequence(seq_pair):
        tokens, extra_part = seq_pair
        forget_pre = lax.optimization_barrier(jnp.dot(tokens, forget_weight, preferred_element_type=jnp.float32).astype(jnp.bfloat16)).astype(jnp.float32)
        values = lax.optimization_barrier(jnp.dot(tokens, value_weight, preferred_element_type=jnp.float32).astype(jnp.bfloat16)).astype(jnp.float32)
        log_forget = jnp.logaddexp(log_lower, log_upper + jax.nn.log_sigmoid(forget_pre)) + extra_part
        key_rows = opening * jax.nn.sigmoid(-forget_pre)
        running = jnp.cumsum(log_forget.reshape(block_count, SPAN, W), axis=1)
        totals = running[:, -1]
        weighted = key_rows.reshape(block_count, SPAN, W) * jnp.exp(totals[:, None] - running)
        weighted = lax.optimization_barrier(weighted.astype(jnp.bfloat16)).astype(jnp.float32)
        weighted = weighted.reshape(block_count, SPAN, head_count, HD)
        value_rows = values.reshape(block_count, SPAN, head_count, HD)
        block_state = jnp.einsum('nthd,nthe->nhde', weighted, value_rows, precision=lax.Precision.HIGHEST)
        later_sum = jnp.cumsum(totals[::-1], axis=0)[::-1] - totals
        end_scale = jnp.exp(later_sum).reshape(block_count, head_count, HD)
        return lax.optimization_barrier(jnp.sum(end_scale[..., None] * block_state, axis=0))
    final_state = lax.map(one_sequence, (prompt, extra_decay))
    state_cache = final_state.transpose(2, 1, 0, 3).astype(jnp.bfloat16)
    new_forget = lax.optimization_barrier(jnp.dot(new_token, forget_weight, preferred_element_type=jnp.float32).astype(jnp.bfloat16)).astype(jnp.float32)
    new_value = lax.optimization_barrier(jnp.dot(new_token, value_weight, preferred_element_type=jnp.float32).astype(jnp.bfloat16)).astype(jnp.float32)
    new_log = jnp.logaddexp(log_lower, log_upper + jax.nn.log_sigmoid(new_forget))
    new_key = opening * jax.nn.sigmoid(-new_forget)
    query_act = jax.nn.silu(new_query.astype(jnp.float32)).reshape(PROMPT_COUNT, head_count, HD)
    updated = jnp.exp(new_log).reshape(PROMPT_COUNT, head_count, HD)[..., None] * final_state
    updated = updated + new_key.reshape(PROMPT_COUNT, head_count, HD)[..., None] * new_value.reshape(PROMPT_COUNT, head_count, 1, HD)
    raw_read = lax.optimization_barrier(jnp.sum(query_act[..., None] * updated, axis=2))
    normed = raw_read * lax.rsqrt(lax.optimization_barrier(jnp.mean(raw_read * raw_read, axis=-1, keepdims=True)) + 1e-06) * read_gain
    first_read = normed.reshape(PROMPT_COUNT, W).astype(jnp.bfloat16)
    return (state_cache, first_read)
```

```python
import jax
import jax.numpy as jnp
from jax import lax
from jax.sharding import PartitionSpec as P

HD = 128


def from_everyone(array, axis):
    devices = lax.axis_size(axis)
    return lax.all_to_all(
        jnp.broadcast_to(array[None], (devices, *array.shape)), axis, 0, 0, tiled=True
    )


def local(
    prompt, forget_weight, value_weight, lower_bound, extra_decay, new_token, new_query, read_gain
):
    seq_count, span_len, _ = prompt.shape
    width_dev = forget_weight.shape[1]
    head_count = width_dev // HD
    blocks = lax.axis_size("sp")
    row_share = HD // blocks
    rows = head_count * seq_count * row_share
    block = lax.axis_index("sp")
    log_lower = jnp.log(lower_bound)
    log_upper = jnp.log1p(-lower_bound)
    opening = 1.0 - lower_bound
    forget_pre = jnp.einsum(
        "std,dw->stw", prompt, forget_weight, preferred_element_type=jnp.float32
    ).astype(jnp.bfloat16)
    values = jnp.einsum(
        "std,dw->stw", prompt, value_weight, preferred_element_type=jnp.float32
    ).astype(jnp.bfloat16)
    forget_wide = lax.optimization_barrier(forget_pre).astype(jnp.float32)
    log_forget = jnp.logaddexp(log_lower, log_upper + jax.nn.log_sigmoid(forget_wide)) + extra_decay
    key_rows = opening * jax.nn.sigmoid(-forget_wide)
    running = jnp.cumsum(log_forget, axis=1)
    totals = running[:, -1]
    weighted = (key_rows * jnp.exp(totals[:, None] - running)).astype(jnp.bfloat16)
    weighted = weighted.reshape(seq_count, span_len, head_count, HD)
    value_rows = values.reshape(seq_count, span_len, head_count, HD)
    block_state = jnp.einsum(
        "sthd,sthe->hsde", weighted, value_rows, preferred_element_type=jnp.float32
    )
    sent = block_state.reshape(head_count, seq_count, blocks, row_share, HD)
    sent = sent.transpose(2, 0, 1, 3, 4).reshape(blocks, rows, HD)
    sent_totals = totals.reshape(seq_count, head_count, blocks, row_share)
    sent_totals = sent_totals.transpose(2, 1, 0, 3).reshape(blocks, 1, rows)
    sent_totals = jnp.pad(sent_totals, ((0, 0), (0, 0), (0, HD - rows)))
    got = lax.all_to_all(jnp.concatenate([sent, sent_totals], 1), "sp", 0, 0, tiled=True)
    got_totals = got[:, rows, :rows]
    later = jnp.arange(blocks)[:, None] < jnp.arange(blocks)[None, :]
    later_sum = jnp.sum(jnp.where(later[:, :, None], got_totals[None], 0.0), axis=1)
    final = jnp.sum(jnp.exp(later_sum)[..., None] * got[:, :rows], axis=0)
    final = final.reshape(head_count, seq_count, row_share, HD)
    state_cache = final.transpose(2, 0, 1, 3).astype(jnp.bfloat16)

    pieces = from_everyone(new_token, "tp")
    whole_token = pieces.transpose(1, 0, 2).reshape(seq_count, -1)
    new_forget = lax.optimization_barrier(
        jnp.dot(whole_token, forget_weight, preferred_element_type=jnp.float32).astype(jnp.bfloat16)
    ).astype(jnp.float32)
    new_value = lax.optimization_barrier(
        jnp.dot(whole_token, value_weight, preferred_element_type=jnp.float32).astype(jnp.bfloat16)
    ).astype(jnp.float32)
    new_log = jnp.logaddexp(log_lower, log_upper + jax.nn.log_sigmoid(new_forget))
    new_key = opening * jax.nn.sigmoid(-new_forget)
    query_act = jax.nn.silu(new_query.astype(jnp.float32))

    def own(array):
        parts = array.reshape(seq_count, head_count, blocks, row_share)
        return lax.dynamic_index_in_dim(parts, block, 2, keepdims=False).transpose(1, 0, 2)

    share = jnp.sum(own(query_act * jnp.exp(new_log))[..., None] * final, axis=2)
    shares = from_everyone(share.reshape(head_count * seq_count, HD), "sp")
    raw_read = jnp.sum(shares, axis=0).reshape(head_count, seq_count, HD).transpose(1, 0, 2)
    key_sum = jnp.sum((query_act * new_key).reshape(seq_count, head_count, HD), axis=-1)
    raw_read = raw_read + key_sum[..., None] * new_value.reshape(seq_count, head_count, HD)
    normed = (
        raw_read
        * lax.rsqrt(jnp.mean(raw_read * raw_read, axis=-1, keepdims=True) + 1e-06)
        * read_gain
    )
    first_read = normed.reshape(seq_count, width_dev).astype(jnp.bfloat16)
    return (state_cache, first_read)


def solution(mesh):
    return jax.shard_map(
        local,
        mesh=mesh,
        in_specs=(
            P(None, "sp", None),
            P(None, "tp"),
            P(None, "tp"),
            P("tp"),
            P(None, "sp", "tp"),
            P(None, "tp"),
            P(None, "tp"),
            P(),
        ),
        out_specs=(P("sp", "tp", None, None), P(None, "tp")),
        check_vma=False,
    )
```

```python
import functools

import jax
import jax.numpy as jnp
from jax import lax
from jax.experimental import pallas as pl
from jax.experimental.pallas import tpu as pltpu
from jax.sharding import PartitionSpec as P

HD = 128
PIECES = 4


def log1p_minus(key):
    poly = jnp.float32(1.0 / 7.0)
    for order in range(6, 0, -1):
        poly = poly * key + jnp.float32(1.0 / order)
    return -(key * poly)


def key_of(forget_pre, opening):
    return opening / (1.0 + jnp.exp(forget_pre))


def dense_kernel(
    prompt, forget_weight, value_weight, lower_bound, extra_decay, sent,
    tokens, forget_w, value_w, extra, tot, first_sems, token_sems, extra_sem,
):
    seq_count, span_len, width = tokens.shape
    dests = sent.shape[0]
    row_share = HD // dests
    head_count = forget_w.shape[1] // HD
    groups = head_count * seq_count
    piece = width // PIECES
    first = []
    for p in range(PIECES):
        cut = pl.ds(p * piece, piece)
        first.append((
            pltpu.make_async_copy(prompt.at[0, :, cut], tokens.at[0, :, cut], first_sems.at[p, 0]),
            pltpu.make_async_copy(forget_weight.at[cut], forget_w.at[cut], first_sems.at[p, 1]),
            pltpu.make_async_copy(value_weight.at[cut], value_w.at[cut], first_sems.at[p, 2]),
        ))
    rest = [
        pltpu.make_async_copy(prompt.at[s], tokens.at[s], token_sems.at[s])
        for s in range(1, seq_count)
    ]
    extra_copy = pltpu.make_async_copy(extra_decay, extra, extra_sem)
    for copies in first:
        for copy in copies:
            copy.start()
    extra_copy.start()
    for copy in rest:
        copy.start()

    opening = 1.0 - lower_bound[...]
    row = lax.broadcasted_iota(jnp.int32, (span_len, span_len), 0)
    col = lax.broadcasted_iota(jnp.int32, (span_len, span_len), 1)
    after = jnp.where(col > row, 1.0, 0.0).astype(jnp.bfloat16)

    def finish(s, forget_pre, values):
        key = key_of(forget_pre.astype(jnp.float32), opening)
        log_forget = log1p_minus(key) + extra[s]
        high = log_forget.astype(jnp.bfloat16)
        left = log_forget - high.astype(jnp.float32)
        middle = left.astype(jnp.bfloat16)
        low = (left - middle.astype(jnp.float32)).astype(jnp.bfloat16)
        later = (
            jnp.dot(after, high, preferred_element_type=jnp.float32)
            + jnp.dot(after, middle, preferred_element_type=jnp.float32)
            + jnp.dot(after, low, preferred_element_type=jnp.float32)
        )
        totals = later[:1] + log_forget[:1]
        weighted = (key * jnp.exp(later)).astype(jnp.bfloat16)
        for h in range(head_count):
            cut = slice(h * HD, (h + 1) * HD)
            group = h * seq_count + s
            tot[group : group + 1, :] = totals[:, cut]
            state = lax.dot_general(
                weighted[:, cut], values[:, cut], (((0,), (0,)), ((), ())),
                preferred_element_type=jnp.float32,
            )
            for k in range(dests):
                sent[k, pl.ds(group, row_share, stride=groups), :] = state[
                    k * row_share : (k + 1) * row_share
                ]

    forget_sum = value_sum = None
    for p in range(PIECES):
        for copy in first[p]:
            copy.wait()
        cut = slice(p * piece, (p + 1) * piece)
        part = tokens[0, :, cut]
        forget_part = jnp.dot(part, forget_w[cut], preferred_element_type=jnp.float32)
        value_part = jnp.dot(part, value_w[cut], preferred_element_type=jnp.float32)
        forget_sum = forget_part if p == 0 else forget_sum + forget_part
        value_sum = value_part if p == 0 else value_sum + value_part
    pending = (forget_sum.astype(jnp.bfloat16), value_sum.astype(jnp.bfloat16))
    extra_copy.wait()
    for s in range(1, seq_count):
        rest[s - 1].wait()
        forget_pre = jnp.dot(
            tokens[s], forget_w[...], preferred_element_type=jnp.float32
        ).astype(jnp.bfloat16)
        values = jnp.dot(
            tokens[s], value_w[...], preferred_element_type=jnp.float32
        ).astype(jnp.bfloat16)
        finish(s - 1, *pending)
        pending = (forget_pre, values)
    finish(seq_count - 1, *pending)
    for k in range(dests):
        sent[k, row_share * groups :, :] = tot[...]


def token_kernel(
    pieces, forget_weight, value_weight, lower_bound, new_query, reach, addend, forget_sum, value_sum
):
    step = pl.program_id(0)
    seq_count = pieces.shape[1]
    head_count = forget_weight.shape[1] // HD

    @pl.when(step == 0)
    def _():
        forget_sum[...] = jnp.zeros_like(forget_sum)
        value_sum[...] = jnp.zeros_like(value_sum)

    forget_sum[...] += jnp.dot(pieces[0], forget_weight[...], preferred_element_type=jnp.float32)
    value_sum[...] += jnp.dot(pieces[0], value_weight[...], preferred_element_type=jnp.float32)

    @pl.when(step == pl.num_programs(0) - 1)
    def _():
        def grouped(rows):
            return jnp.concatenate(
                [rows[:, h * HD : (h + 1) * HD] for h in range(head_count)], axis=0
            )

        new_forget = forget_sum[...].astype(jnp.bfloat16).astype(jnp.float32)
        new_value = grouped(value_sum[...].astype(jnp.bfloat16).astype(jnp.float32))
        new_key = key_of(new_forget, 1.0 - lower_bound[...])
        query = new_query[...].astype(jnp.float32)
        query = query / (1.0 + jnp.exp(-query))
        reach[...] = grouped(query * (1.0 - new_key))
        key_sum = jnp.sum(grouped(query * new_key), axis=1, keepdims=True)
        addend[...] = key_sum * new_value


def state_kernel(got, reach, state_cache, shares, *, axis):
    blocks, rows, _ = got.shape
    groups = reach.shape[0]
    row_share = HD // blocks
    head_count, seq_count = state_cache.shape[1:3]
    back = lax.rem(HD - lax.axis_index(axis) * row_share, HD)
    final = [None] * row_share
    later = jnp.zeros((groups, HD), jnp.float32)
    for b in range(blocks - 1, -1, -1):
        scale = pltpu.roll(jnp.exp(later), back, 1)
        for d in range(row_share):
            term = scale[:, d : d + 1] * got[b, d * groups : (d + 1) * groups, :]
            final[d] = term if final[d] is None else final[d] + term
        if b > 0:
            later = later + got[b, row_share * groups :, :]
    own_reach = pltpu.roll(reach[...], back, 1)
    share = None
    for d in range(row_share):
        for h in range(head_count):
            state_cache[d, h] = final[d][h * seq_count : (h + 1) * seq_count].astype(jnp.bfloat16)
        term = own_reach[:, d : d + 1] * final[d]
        share = term if share is None else share + term
    for k in range(blocks):
        shares[k] = share


def read_kernel(shares, addend, read_gain, first_read):
    blocks = shares.shape[0]
    seq_count = first_read.shape[0]
    raw = shares[0]
    for k in range(1, blocks):
        raw = raw + shares[k]
    raw = raw + addend[...]
    mean = jnp.mean(raw * raw, axis=1, keepdims=True)
    normed = raw * lax.rsqrt(mean + 1e-06) * read_gain[...]
    for h in range(first_read.shape[1] // HD):
        first_read[:, h * HD : (h + 1) * HD] = normed[
            h * seq_count : (h + 1) * seq_count
        ].astype(jnp.bfloat16)


def local(
    prompt, forget_weight, value_weight, lower_bound, extra_decay, new_token, new_query, read_gain
):
    seq_count, span_len, width = prompt.shape
    width_dev = forget_weight.shape[1]
    head_count = width_dev // HD
    blocks = lax.axis_size("sp")
    peers = lax.axis_size("tp")
    row_share = HD // blocks
    groups = head_count * seq_count
    rows = (row_share + 1) * groups
    anywhere = pl.BlockSpec(memory_space=pl.ANY)
    vmem = pl.BlockSpec(memory_space=pltpu.VMEM)
    lower_row = lower_bound[None]
    sent = pl.pallas_call(
        dense_kernel,
        out_shape=jax.ShapeDtypeStruct((blocks, rows, HD), jnp.float32),
        in_specs=[anywhere, anywhere, anywhere, vmem, anywhere],
        out_specs=vmem,
        scratch_shapes=[
            pltpu.VMEM((seq_count, span_len, width), jnp.bfloat16),
            pltpu.VMEM((width, width_dev), jnp.bfloat16),
            pltpu.VMEM((width, width_dev), jnp.bfloat16),
            pltpu.VMEM((seq_count, span_len, width_dev), jnp.float32),
            pltpu.VMEM((groups, HD), jnp.float32),
            pltpu.SemaphoreType.DMA((PIECES, 3)),
            pltpu.SemaphoreType.DMA((seq_count,)),
            pltpu.SemaphoreType.DMA,
        ],
        name="dense",
    )(prompt, forget_weight, value_weight, lower_row, extra_decay)
    got = lax.all_to_all(sent, "sp", 0, 0, tiled=True)

    token, _ = lax.optimization_barrier((new_token, sent))
    pieces = lax.all_to_all(
        jnp.broadcast_to(token[None], (peers, *token.shape)), "tp", 0, 0, tiled=True
    )
    part = width // peers
    reach, addend = pl.pallas_call(
        token_kernel,
        grid=(peers,),
        out_shape=[jax.ShapeDtypeStruct((groups, HD), jnp.float32)] * 2,
        in_specs=[
            pl.BlockSpec((1, seq_count, part), lambda i: (i, 0, 0)),
            pl.BlockSpec((part, width_dev), lambda i: (i, 0)),
            pl.BlockSpec((part, width_dev), lambda i: (i, 0)),
            pl.BlockSpec((1, width_dev), lambda i: (0, 0)),
            pl.BlockSpec((seq_count, width_dev), lambda i: (0, 0)),
        ],
        out_specs=[pl.BlockSpec((groups, HD), lambda i: (0, 0))] * 2,
        scratch_shapes=[pltpu.VMEM((seq_count, width_dev), jnp.float32)] * 2,
        name="token",
    )(pieces, forget_weight, value_weight, lower_row, new_query)
    state_cache, shares = pl.pallas_call(
        functools.partial(state_kernel, axis="sp"),
        out_shape=[
            jax.ShapeDtypeStruct((row_share, head_count, seq_count, HD), jnp.bfloat16),
            jax.ShapeDtypeStruct((blocks, groups, HD), jnp.float32),
        ],
        in_specs=[vmem, vmem],
        out_specs=[vmem, vmem],
        name="state",
    )(got, reach)
    shares = lax.all_to_all(shares, "sp", 0, 0, tiled=True)
    first_read = pl.pallas_call(
        read_kernel,
        out_shape=jax.ShapeDtypeStruct((seq_count, width_dev), jnp.bfloat16),
        in_specs=[vmem, vmem, vmem],
        out_specs=vmem,
        name="read",
    )(shares, addend, read_gain[None])
    return (state_cache, first_read)


def solution(mesh):
    return jax.shard_map(
        local,
        mesh=mesh,
        in_specs=(
            P(None, "sp", None),
            P(None, "tp"),
            P(None, "tp"),
            P("tp"),
            P(None, "sp", "tp"),
            P(None, "tp"),
            P(None, "tp"),
            P(),
        ),
        out_specs=(P("sp", "tp", None, None), P(None, "tp")),
        check_vma=False,
    )
```

```python
import functools

import jax
import jax.numpy as jnp
from jax import lax
from jax.experimental import pallas as pl
from jax.experimental.pallas import tpu as pltpu
from jax.sharding import PartitionSpec as P

HD = 128
PIECES = 4


def log1p_minus(key):
    poly = jnp.float32(1.0 / 7.0)
    for order in range(6, 0, -1):
        poly = poly * key + jnp.float32(1.0 / order)
    return -(key * poly)


def key_of(forget_pre, opening):
    return opening / (1.0 + jnp.exp(forget_pre))


def dense_kernel(
    prompt, forget_weight, value_weight, lower_bound, extra_decay, sent,
    tokens, forget_w, value_w, extra, lower, tot, first_sems, token_sems, extra_sem, lower_sem,
):
    seq_count, span_len, width = tokens.shape
    dests = sent.shape[0]
    row_share = HD // dests
    head_count = forget_w.shape[1] // HD
    groups = head_count * seq_count
    piece = width // PIECES
    first = []
    for p in range(PIECES):
        cut = pl.ds(p * piece, piece)
        first.append((
            pltpu.make_async_copy(prompt.at[0, :, cut], tokens.at[0, :, cut], first_sems.at[p, 0]),
            pltpu.make_async_copy(forget_weight.at[cut], forget_w.at[cut], first_sems.at[p, 1]),
            pltpu.make_async_copy(value_weight.at[cut], value_w.at[cut], first_sems.at[p, 2]),
        ))
    rest = [
        pltpu.make_async_copy(prompt.at[s], tokens.at[s], token_sems.at[s])
        for s in range(1, seq_count)
    ]
    extra_copy = pltpu.make_async_copy(extra_decay, extra, extra_sem)
    lower_copy = pltpu.make_async_copy(lower_bound, lower, lower_sem)
    lower_copy.start()
    for copies in first:
        for copy in copies:
            copy.start()
    extra_copy.start()
    for copy in rest:
        copy.start()

    row = lax.broadcasted_iota(jnp.int32, (span_len, span_len), 0)
    col = lax.broadcasted_iota(jnp.int32, (span_len, span_len), 1)
    after = jnp.where(col > row, 1.0, 0.0).astype(jnp.bfloat16)

    def finish(s, forget_pre, values):
        key = key_of(forget_pre.astype(jnp.float32), opening)
        log_forget = log1p_minus(key) + extra[s]
        high = log_forget.astype(jnp.bfloat16)
        left = log_forget - high.astype(jnp.float32)
        middle = left.astype(jnp.bfloat16)
        low = (left - middle.astype(jnp.float32)).astype(jnp.bfloat16)
        later = (
            jnp.dot(after, high, preferred_element_type=jnp.float32)
            + jnp.dot(after, middle, preferred_element_type=jnp.float32)
            + jnp.dot(after, low, preferred_element_type=jnp.float32)
        )
        totals = later[:1] + log_forget[:1]
        weighted = (key * jnp.exp(later)).astype(jnp.bfloat16)
        for h in range(head_count):
            cut = slice(h * HD, (h + 1) * HD)
            group = h * seq_count + s
            tot[group : group + 1, :] = totals[:, cut]
            state = lax.dot_general(
                weighted[:, cut], values[:, cut], (((0,), (0,)), ((), ())),
                preferred_element_type=jnp.float32,
            )
            for k in range(dests):
                sent[k, pl.ds(group, row_share, stride=groups), :] = state[
                    k * row_share : (k + 1) * row_share
                ]

    forget_sum = value_sum = None
    for p in range(PIECES):
        for copy in first[p]:
            copy.wait()
        cut = slice(p * piece, (p + 1) * piece)
        part = tokens[0, :, cut]
        forget_part = jnp.dot(part, forget_w[cut], preferred_element_type=jnp.float32)
        value_part = jnp.dot(part, value_w[cut], preferred_element_type=jnp.float32)
        forget_sum = forget_part if p == 0 else forget_sum + forget_part
        value_sum = value_part if p == 0 else value_sum + value_part
    pending = (forget_sum.astype(jnp.bfloat16), value_sum.astype(jnp.bfloat16))
    extra_copy.wait()
    lower_copy.wait()
    opening = 1.0 - lower[...]
    for s in range(1, seq_count):
        rest[s - 1].wait()
        forget_pre = jnp.dot(
            tokens[s], forget_w[...], preferred_element_type=jnp.float32
        ).astype(jnp.bfloat16)
        values = jnp.dot(
            tokens[s], value_w[...], preferred_element_type=jnp.float32
        ).astype(jnp.bfloat16)
        finish(s - 1, *pending)
        pending = (forget_pre, values)
    finish(seq_count - 1, *pending)
    for k in range(dests):
        sent[k, row_share * groups :, :] = tot[...]


def token_kernel(
    own, pair, far, forget_weight, value_weight, lower_bound, new_query, reach, addend,
    forget_w, value_w, whole, sems, *, axis
):
    copies = [
        pltpu.make_async_copy(forget_weight, forget_w, sems.at[0]),
        pltpu.make_async_copy(value_weight, value_w, sems.at[1]),
    ]
    for copy in copies:
        copy.start()
    _, part = own.shape
    peers = whole.shape[1] // part
    head_count = forget_w.shape[1] // HD
    me = lax.axis_index(axis)
    held = [(me, own[...]), (me ^ 1, pair[...])]
    for step in range(1, peers // 2):
        source = lax.rem(me + peers - 2 * step, peers)
        held += [(source, far[step - 1, 0]), (source ^ 1, far[step - 1, 1])]
    for source, rows in held:
        whole[:, pl.ds(pl.multiple_of(source * part, part), part)] = rows.astype(jnp.float32)
    token = whole[...].astype(jnp.bfloat16)
    for copy in copies:
        copy.wait()

    def grouped(rows):
        return jnp.concatenate([rows[:, h * HD : (h + 1) * HD] for h in range(head_count)], axis=0)

    def rounded(weight):
        out = jnp.dot(token, weight[...], preferred_element_type=jnp.float32)
        return out.astype(jnp.bfloat16).astype(jnp.float32)

    new_key = key_of(rounded(forget_w), 1.0 - lower_bound[...])
    query = new_query[...].astype(jnp.float32)
    query = query / (1.0 + jnp.exp(-query))
    reach[...] = grouped(query * (1.0 - new_key))
    key_sum = jnp.sum(grouped(query * new_key), axis=1, keepdims=True)
    addend[...] = key_sum * grouped(rounded(value_w))


def state_kernel(got, reach, state_cache, shares, *, axis):
    blocks, _, _ = got.shape
    groups = reach.shape[0]
    row_share = HD // blocks
    head_count, seq_count = state_cache.shape[1:3]
    back = lax.rem(HD - lax.axis_index(axis) * row_share, HD)
    final = [None] * row_share
    later = jnp.zeros((groups, HD), jnp.float32)
    for b in range(blocks - 1, -1, -1):
        scale = pltpu.roll(jnp.exp(later), back, 1)
        for d in range(row_share):
            term = scale[:, d : d + 1] * got[b, d * groups : (d + 1) * groups, :]
            final[d] = term if final[d] is None else final[d] + term
        if b > 0:
            later = later + got[b, row_share * groups :, :]
    own_reach = pltpu.roll(reach[...], back, 1)
    share = None
    for d in range(row_share):
        for h in range(head_count):
            state_cache[d, h] = final[d][h * seq_count : (h + 1) * seq_count].astype(jnp.bfloat16)
        term = own_reach[:, d : d + 1] * final[d]
        share = term if share is None else share + term
    for k in range(blocks):
        shares[k] = share


def read_kernel(shares, addend, read_gain, first_read):
    blocks = shares.shape[0]
    seq_count = first_read.shape[0]
    raw = shares[0]
    for k in range(1, blocks):
        raw = raw + shares[k]
    raw = raw + addend[...]
    mean = jnp.mean(raw * raw, axis=1, keepdims=True)
    normed = raw * lax.rsqrt(mean + 1e-06) * read_gain[...]
    for h in range(first_read.shape[1] // HD):
        first_read[:, h * HD : (h + 1) * HD] = normed[
            h * seq_count : (h + 1) * seq_count
        ].astype(jnp.bfloat16)


def local(
    prompt, forget_weight, value_weight, lower_bound, extra_decay, new_token, new_query, read_gain
):
    seq_count, span_len, width = prompt.shape
    width_dev = forget_weight.shape[1]
    head_count = width_dev // HD
    blocks = lax.axis_size("sp")
    peers = lax.axis_size("tp")
    row_share = HD // blocks
    groups = head_count * seq_count
    rows = (row_share + 1) * groups
    anywhere = pl.BlockSpec(memory_space=pltpu.HBM)
    vmem = pl.BlockSpec(memory_space=pltpu.VMEM)
    lower_row = lower_bound[None]
    sent = pl.pallas_call(
        dense_kernel,
        out_shape=jax.ShapeDtypeStruct((blocks, rows, HD), jnp.float32),
        in_specs=[anywhere] * 5,
        out_specs=vmem,
        scratch_shapes=[
            pltpu.VMEM((seq_count, span_len, width), jnp.bfloat16),
            pltpu.VMEM((width, width_dev), jnp.bfloat16),
            pltpu.VMEM((width, width_dev), jnp.bfloat16),
            pltpu.VMEM((seq_count, span_len, width_dev), jnp.float32),
            pltpu.VMEM((1, width_dev), jnp.float32),
            pltpu.VMEM((groups, HD), jnp.float32),
            pltpu.SemaphoreType.DMA((PIECES, 3)),
            pltpu.SemaphoreType.DMA((seq_count,)),
            pltpu.SemaphoreType.DMA,
            pltpu.SemaphoreType.DMA,
        ],
        name="dense",
    )(prompt, forget_weight, value_weight, lower_row, extra_decay)
    got = lax.all_to_all(sent, "sp", 0, 0, tiled=True)
    token, _ = lax.optimization_barrier((new_token, sent))
    pair = lax.ppermute(token, "tp", [(i, i ^ 1) for i in range(peers)])
    both = jnp.stack([token, pair])
    far = []
    for step in range(1, peers // 2):
        far.append(lax.ppermute(both, "tp", [(i, (i + 2 * step) % peers) for i in range(peers)]))
    reach, addend = pl.pallas_call(
        functools.partial(token_kernel, axis="tp"),
        out_shape=[jax.ShapeDtypeStruct((groups, HD), jnp.float32)] * 2,
        in_specs=[vmem, vmem, vmem, anywhere, anywhere, vmem, vmem],
        out_specs=[vmem] * 2,
        scratch_shapes=[
            pltpu.VMEM((width, width_dev), jnp.bfloat16),
            pltpu.VMEM((width, width_dev), jnp.bfloat16),
            pltpu.VMEM((seq_count, width), jnp.float32),
            pltpu.SemaphoreType.DMA((2,)),
        ],
        name="token",
    )(token, pair, jnp.stack(far), forget_weight, value_weight, lower_row, new_query)
    got = pltpu.with_memory_space_constraint(got, pltpu.VMEM)
    state_cache, shares = pl.pallas_call(
        functools.partial(state_kernel, axis="sp"),
        out_shape=[
            jax.ShapeDtypeStruct((row_share, head_count, seq_count, HD), jnp.bfloat16),
            pltpu.VMEM((blocks, groups, HD), jnp.float32),
        ],
        in_specs=[vmem, vmem],
        out_specs=[vmem, vmem],
        name="state",
    )(got, reach)
    shares = pltpu.with_memory_space_constraint(lax.all_to_all(shares, "sp", 0, 0, tiled=True), pltpu.VMEM)
    first_read = pl.pallas_call(
        read_kernel,
        out_shape=jax.ShapeDtypeStruct((seq_count, width_dev), jnp.bfloat16),
        in_specs=[vmem, vmem, vmem],
        out_specs=vmem,
        name="read",
    )(shares, addend, read_gain[None])
    return (state_cache, first_read)


def solution(mesh):
    return jax.shard_map(
        local,
        mesh=mesh,
        in_specs=(
            P(None, "sp", None),
            P(None, "tp"),
            P(None, "tp"),
            P("tp"),
            P(None, "sp", "tp"),
            P(None, "tp"),
            P(None, "tp"),
            P(),
        ),
        out_specs=(P("sp", "tp", None, None), P(None, "tp")),
        check_vma=False,
    )
```

```python
import functools

import jax
import jax.numpy as jnp
from jax import lax
from jax.experimental import pallas as pl
from jax.experimental.pallas import tpu as pltpu
from jax.sharding import PartitionSpec as P

HD = 128
PIECES = 4
AHEAD = 5


def log1p_minus(key):
    poly = jnp.float32(1.0 / 7.0)
    for order in range(6, 0, -1):
        poly = poly * key + jnp.float32(1.0 / order)
    return -(key * poly)


def key_of(forget_pre, opening):
    return opening / (1.0 + jnp.exp(forget_pre))


def dense_kernel(
    prompt, forget_weight, value_weight, lower_bound, extra_decay, sent,
    tokens, forget_w, value_w, extra, lower, tot, sems,
):
    seq_count, span_len, width = tokens.shape
    dests = sent.shape[0]
    row_share = HD // dests
    head_count = forget_w.shape[1] // HD
    groups = head_count * seq_count
    piece = width // PIECES
    groups_in = []

    def group(*pairs):
        base = sum(len(copies) for copies in groups_in)
        groups_in.append([
            pltpu.make_async_copy(source, target, sems.at[base + i])
            for i, (source, target) in enumerate(pairs)
        ])

    for p in range(PIECES):
        cut = pl.ds(p * piece, piece)
        group(
            (prompt.at[0, :, cut], tokens.at[0, :, cut]),
            (forget_weight.at[cut], forget_w.at[cut]),
            (value_weight.at[cut], value_w.at[cut]),
        )
    half = span_len // 2
    for s in range(1, seq_count):
        pairs = [
            (prompt.at[s, pl.ds(at, half)], tokens.at[s, pl.ds(at, half)]) for at in (0, half)
        ]
        if s == 1:
            pairs += [(extra_decay, extra), (lower_bound, lower)]
        group(*pairs)

    def start(at):
        if at < len(groups_in):
            for copy in groups_in[at]:
                copy.start()

    def arrive(at):
        for copy in groups_in[at]:
            copy.wait()
        start(at + AHEAD)

    for at in range(AHEAD):
        start(at)

    row = lax.broadcasted_iota(jnp.int32, (span_len, span_len), 0)
    col = lax.broadcasted_iota(jnp.int32, (span_len, span_len), 1)
    after = jnp.where(col > row, 1.0, 0.0).astype(jnp.bfloat16)

    def finish(s, opening, forget_pre, values):
        key = key_of(forget_pre.astype(jnp.float32), opening)
        log_forget = log1p_minus(key) + extra[s]
        high = log_forget.astype(jnp.bfloat16)
        left = log_forget - high.astype(jnp.float32)
        middle = left.astype(jnp.bfloat16)
        low = (left - middle.astype(jnp.float32)).astype(jnp.bfloat16)
        later = (
            jnp.dot(after, high, preferred_element_type=jnp.float32)
            + jnp.dot(after, middle, preferred_element_type=jnp.float32)
            + jnp.dot(after, low, preferred_element_type=jnp.float32)
        )
        totals = later[:1] + log_forget[:1]
        weighted = (key * jnp.exp(later)).astype(jnp.bfloat16)
        for h in range(head_count):
            cut = slice(h * HD, (h + 1) * HD)
            group = h * seq_count + s
            tot[group : group + 1, :] = totals[:, cut]
            state = lax.dot_general(
                weighted[:, cut], values[:, cut], (((0,), (0,)), ((), ())),
                preferred_element_type=jnp.float32,
            )
            for k in range(dests):
                sent[k, pl.ds(group, row_share, stride=groups), :] = state[
                    k * row_share : (k + 1) * row_share
                ]

    forget_sum = value_sum = None
    for p in range(PIECES):
        arrive(p)
        cut = slice(p * piece, (p + 1) * piece)
        part = tokens[0, :, cut]
        forget_part = jnp.dot(part, forget_w[cut], preferred_element_type=jnp.float32)
        value_part = jnp.dot(part, value_w[cut], preferred_element_type=jnp.float32)
        forget_sum = forget_part if p == 0 else forget_sum + forget_part
        value_sum = value_part if p == 0 else value_sum + value_part
    pending = (forget_sum.astype(jnp.bfloat16), value_sum.astype(jnp.bfloat16))
    opening = None
    for s in range(1, seq_count):
        arrive(PIECES + s - 1)
        opening = 1.0 - lower[...]
        forget_pre = jnp.dot(
            tokens[s], forget_w[...], preferred_element_type=jnp.float32
        ).astype(jnp.bfloat16)
        values = jnp.dot(
            tokens[s], value_w[...], preferred_element_type=jnp.float32
        ).astype(jnp.bfloat16)
        finish(s - 1, opening, *pending)
        pending = (forget_pre, values)
    finish(seq_count - 1, opening, *pending)
    for k in range(dests):
        sent[k, row_share * groups :, :] = tot[...]


def token_kernel(
    own, pair, *refs, axis
):
    far = refs[:-10]
    forget_weight, value_weight, lower_bound, new_query, reach, addend = refs[-10:-4]
    forget_w, value_w, whole, sems = refs[-4:]
    copies = [
        pltpu.make_async_copy(forget_weight, forget_w, sems.at[0]),
        pltpu.make_async_copy(value_weight, value_w, sems.at[1]),
    ]
    for copy in copies:
        copy.start()
    _, part = own.shape
    peers = whole.shape[1] // part
    head_count = forget_w.shape[1] // HD
    me = lax.axis_index(axis)
    held = [(me, own[...]), (me ^ 1, pair[...])]
    for step in range(1, peers // 2):
        source = lax.rem(me + peers - 2 * step, peers)
        held += [(source, far[step - 1][0]), (source ^ 1, far[step - 1][1])]
    for source, rows in held:
        whole[:, pl.ds(pl.multiple_of(source * part, part), part)] = rows.astype(jnp.float32)
    token = whole[...].astype(jnp.bfloat16)
    for copy in copies:
        copy.wait()

    def grouped(rows):
        return jnp.concatenate([rows[:, h * HD : (h + 1) * HD] for h in range(head_count)], axis=0)

    def rounded(weight):
        out = jnp.dot(token, weight[...], preferred_element_type=jnp.float32)
        return out.astype(jnp.bfloat16).astype(jnp.float32)

    new_key = key_of(rounded(forget_w), 1.0 - lower_bound[...])
    query = new_query[...].astype(jnp.float32)
    query = query / (1.0 + jnp.exp(-query))
    reach[...] = grouped(query * (1.0 - new_key))
    key_sum = jnp.sum(grouped(query * new_key), axis=1, keepdims=True)
    addend[...] = key_sum * grouped(rounded(value_w))


def state_kernel(got, reach, state_cache, shares, *, axis):
    blocks, _, _ = got.shape
    groups = reach.shape[0]
    row_share = HD // blocks
    head_count, seq_count = state_cache.shape[1:3]
    back = lax.rem(HD - lax.axis_index(axis) * row_share, HD)
    final = [None] * row_share
    later = jnp.zeros((groups, HD), jnp.float32)
    for b in range(blocks - 1, -1, -1):
        scale = pltpu.roll(jnp.exp(later), back, 1)
        for d in range(row_share):
            term = scale[:, d : d + 1] * got[b, d * groups : (d + 1) * groups, :]
            final[d] = term if final[d] is None else final[d] + term
        if b > 0:
            later = later + got[b, row_share * groups :, :]
    own_reach = pltpu.roll(reach[...], back, 1)
    share = None
    for d in range(row_share):
        for h in range(head_count):
            state_cache[d, h] = final[d][h * seq_count : (h + 1) * seq_count].astype(jnp.bfloat16)
        term = own_reach[:, d : d + 1] * final[d]
        share = term if share is None else share + term
    for k in range(blocks):
        shares[k] = share


def read_kernel(shares, addend, read_gain, final, state_cache, first_read):
    state_cache[...] = final[...]
    blocks = shares.shape[0]
    seq_count = first_read.shape[0]
    raw = shares[0]
    for k in range(1, blocks):
        raw = raw + shares[k]
    raw = raw + addend[...]
    mean = jnp.mean(raw * raw, axis=1, keepdims=True)
    normed = raw * lax.rsqrt(mean + 1e-06) * read_gain[...]
    for h in range(first_read.shape[1] // HD):
        first_read[:, h * HD : (h + 1) * HD] = normed[
            h * seq_count : (h + 1) * seq_count
        ].astype(jnp.bfloat16)


def near(array):
    return pltpu.with_memory_space_constraint(array, pltpu.VMEM)


def local(
    prompt, forget_weight, value_weight, lower_bound, extra_decay, new_token, new_query, read_gain
):
    seq_count, span_len, width = prompt.shape
    width_dev = forget_weight.shape[1]
    head_count = width_dev // HD
    blocks = lax.axis_size("sp")
    peers = lax.axis_size("tp")
    row_share = HD // blocks
    groups = head_count * seq_count
    rows = (row_share + 1) * groups
    anywhere = pl.BlockSpec(memory_space=pltpu.HBM)
    vmem = pl.BlockSpec(memory_space=pltpu.VMEM)
    lower_row = lower_bound[None]
    sent = pl.pallas_call(
        dense_kernel,
        out_shape=jax.ShapeDtypeStruct((blocks, rows, HD), jnp.float32),
        in_specs=[anywhere] * 5,
        out_specs=vmem,
        scratch_shapes=[
            pltpu.VMEM((seq_count, span_len, width), jnp.bfloat16),
            pltpu.VMEM((width, width_dev), jnp.bfloat16),
            pltpu.VMEM((width, width_dev), jnp.bfloat16),
            pltpu.VMEM((seq_count, span_len, width_dev), jnp.float32),
            pltpu.VMEM((1, width_dev), jnp.float32),
            pltpu.VMEM((groups, HD), jnp.float32),
            pltpu.SemaphoreType.DMA((3 * PIECES + 2 * (seq_count - 1) + 2,)),
        ],
        name="dense",
    )(prompt, forget_weight, value_weight, lower_row, extra_decay)
    got = lax.all_to_all(sent, "sp", 0, 0, tiled=True)
    token, _ = lax.optimization_barrier((new_token, sent))
    pair = lax.ppermute(token, "tp", [(i, i ^ 1) for i in range(peers)])
    both = jnp.stack([token, pair])
    far = []
    for step in range(1, peers // 2):
        far.append(
            lax.ppermute(both, "tp", [(i, (i + 2 * step) % peers) for i in range(peers)])
        )
    reach, addend = pl.pallas_call(
        functools.partial(token_kernel, axis="tp"),
        out_shape=[pltpu.VMEM((groups, HD), jnp.float32)] * 2,
        in_specs=[vmem] * (2 + len(far)) + [anywhere, anywhere, vmem, vmem],
        out_specs=[vmem] * 2,
        scratch_shapes=[
            pltpu.VMEM((width, width_dev), jnp.bfloat16),
            pltpu.VMEM((width, width_dev), jnp.bfloat16),
            pltpu.VMEM((seq_count, width), jnp.float32),
            pltpu.SemaphoreType.DMA((2,)),
        ],
        name="token",
    )(
        near(token), near(pair), *map(near, far), forget_weight, value_weight,
        near(lower_row), near(new_query),
    )
    got = near(got)
    final, shares = pl.pallas_call(
        functools.partial(state_kernel, axis="sp"),
        out_shape=[
            pltpu.VMEM((row_share, head_count, seq_count, HD), jnp.bfloat16),
            pltpu.VMEM((blocks, groups, HD), jnp.float32),
        ],
        in_specs=[vmem, vmem],
        out_specs=[vmem, vmem],
        name="state",
    )(got, near(reach))
    shares = near(lax.all_to_all(shares, "sp", 0, 0, tiled=True))
    state_cache, first_read = pl.pallas_call(
        read_kernel,
        out_shape=[
            jax.ShapeDtypeStruct(final.shape, final.dtype),
            jax.ShapeDtypeStruct((seq_count, width_dev), jnp.bfloat16),
        ],
        in_specs=[vmem] * 4,
        out_specs=[vmem] * 2,
        name="read",
    )(shares, near(addend), near(read_gain[None]), near(final))
    return (state_cache, first_read)


def solution(mesh):
    return jax.shard_map(
        local,
        mesh=mesh,
        in_specs=(
            P(None, "sp", None),
            P(None, "tp"),
            P(None, "tp"),
            P("tp"),
            P(None, "sp", "tp"),
            P(None, "tp"),
            P(None, "tp"),
            P(),
        ),
        out_specs=(P("sp", "tp", None, None), P(None, "tp")),
        check_vma=False,
    )
```

```python
import functools

import jax
import jax.numpy as jnp
from jax import lax
from jax.experimental import pallas as pl
from jax.experimental.pallas import tpu as pltpu
from jax.sharding import PartitionSpec as P

HD = 128
PIECES = 4
AHEAD = 5


def log1p_minus(key):
    poly = jnp.float32(1.0 / 7.0)
    for order in range(6, 0, -1):
        poly = poly * key + jnp.float32(1.0 / order)
    return -(key * poly)


def key_of(forget_pre, opening):
    return opening / (1.0 + jnp.exp(forget_pre))


def dense_kernel(
    prompt, forget_weight, value_weight, lower_bound, extra_decay, sent,
    tokens, forget_w, value_w, extra, lower, tot, sems,
):
    seq_count, span_len, width = tokens.shape
    dests = sent.shape[0]
    row_share = HD // dests
    head_count = forget_w.shape[1] // HD
    groups = head_count * seq_count
    piece = width // PIECES
    groups_in = []

    def group(*pairs):
        base = sum(len(copies) for copies in groups_in)
        groups_in.append([
            pltpu.make_async_copy(source, target, sems.at[base + i])
            for i, (source, target) in enumerate(pairs)
        ])

    for p in range(PIECES):
        cut = pl.ds(p * piece, piece)
        group(
            (prompt.at[0, :, cut], tokens.at[0, :, cut]),
            (forget_weight.at[cut], forget_w.at[cut]),
            (value_weight.at[cut], value_w.at[cut]),
        )
    half = span_len // 2
    for s in range(1, seq_count):
        pairs = [
            (prompt.at[s, pl.ds(at, half)], tokens.at[s, pl.ds(at, half)]) for at in (0, half)
        ]
        if s == 1:
            pairs += [(extra_decay, extra), (lower_bound, lower)]
        group(*pairs)

    def start(at):
        if at < len(groups_in):
            for copy in groups_in[at]:
                copy.start()

    def arrive(at):
        for copy in groups_in[at]:
            copy.wait()
        start(at + AHEAD)

    for at in range(AHEAD):
        start(at)

    row = lax.broadcasted_iota(jnp.int32, (span_len, span_len), 0)
    col = lax.broadcasted_iota(jnp.int32, (span_len, span_len), 1)
    after = jnp.where(col > row, 1.0, 0.0).astype(jnp.bfloat16)

    lane = lax.broadcasted_iota(jnp.int32, (HD, HD), 1)
    powers = [jnp.zeros((HD, HD), jnp.float32)]

    def finish(s, opening, forget_pre, values):
        key = key_of(forget_pre.astype(jnp.float32), opening)
        log_forget = log1p_minus(key) + extra[s]
        high = log_forget.astype(jnp.bfloat16)
        left = log_forget - high.astype(jnp.float32)
        middle = left.astype(jnp.bfloat16)
        low = (left - middle.astype(jnp.float32)).astype(jnp.bfloat16)
        later = (
            jnp.dot(after, high, preferred_element_type=jnp.float32)
            + jnp.dot(after, middle, preferred_element_type=jnp.float32)
            + jnp.dot(after, low, preferred_element_type=jnp.float32)
        )
        totals = later[:1] + log_forget[:1]
        weighted = (key * jnp.exp(later)).astype(jnp.bfloat16)
        for h in range(head_count):
            cut = slice(h * HD, (h + 1) * HD)
            group = h * seq_count + s
            tot[group : group + 1, :] = totals[:, cut]
            state = lax.dot_general(
                weighted[:, cut], values[:, cut], (((0,), (0,)), ((), ())),
                preferred_element_type=jnp.float32,
            )
            peak = jnp.max(jnp.abs(state), axis=1, keepdims=True)
            power = jnp.ceil(jnp.log2(jnp.maximum(peak, 1e-30)))
            state = state * jnp.exp2(-power)
            powers[0] = jnp.where(lane == group, power, powers[0])
            for k in range(dests):
                sent[k, pl.ds(group, row_share, stride=groups), :] = state[
                    k * row_share : (k + 1) * row_share
                ]

    forget_sum = value_sum = None
    for p in range(PIECES):
        arrive(p)
        cut = slice(p * piece, (p + 1) * piece)
        part = tokens[0, :, cut]
        forget_part = jnp.dot(part, forget_w[cut], preferred_element_type=jnp.float32)
        value_part = jnp.dot(part, value_w[cut], preferred_element_type=jnp.float32)
        forget_sum = forget_part if p == 0 else forget_sum + forget_part
        value_sum = value_part if p == 0 else value_sum + value_part
    pending = (forget_sum.astype(jnp.bfloat16), value_sum.astype(jnp.bfloat16))
    opening = None
    for s in range(1, seq_count):
        arrive(PIECES + s - 1)
        opening = 1.0 - lower[...]
        forget_pre = jnp.dot(
            tokens[s], forget_w[...], preferred_element_type=jnp.float32
        ).astype(jnp.bfloat16)
        values = jnp.dot(
            tokens[s], value_w[...], preferred_element_type=jnp.float32
        ).astype(jnp.bfloat16)
        finish(s - 1, opening, *pending)
        pending = (forget_pre, values)
    finish(seq_count - 1, opening, *pending)
    total = tot[...]
    high = total.astype(jnp.bfloat16).astype(jnp.float32)
    left = total - high
    middle = left.astype(jnp.bfloat16).astype(jnp.float32)
    parts = (high, middle, left - middle, powers[0].T[:groups])
    at = lax.broadcasted_iota(jnp.int32, (groups, HD), 1) // row_share
    for k in range(dests):
        tile = None
        for i, part in enumerate(parts):
            turned = pltpu.roll(part, (HD + (i - k) * row_share) % HD, 1)
            tile = turned if tile is None else jnp.where(at == i, turned, tile)
        sent[k, row_share * groups :, :] = tile


def token_kernel(
    own, pair, *refs, axis
):
    far = refs[:-10]
    forget_weight, value_weight, lower_bound, new_query, reach, addend = refs[-10:-4]
    forget_w, value_w, whole, sems = refs[-4:]
    copies = [
        pltpu.make_async_copy(forget_weight, forget_w, sems.at[0]),
        pltpu.make_async_copy(value_weight, value_w, sems.at[1]),
    ]
    for copy in copies:
        copy.start()
    _, part = own.shape
    peers = whole.shape[1] // part
    head_count = forget_w.shape[1] // HD
    me = lax.axis_index(axis)
    held = [(me, own[...]), (me ^ 1, pair[...])]
    for step in range(1, peers // 2):
        source = lax.rem(me + peers - 2 * step, peers)
        held += [(source, far[step - 1][0]), (source ^ 1, far[step - 1][1])]
    for source, rows in held:
        whole[:, pl.ds(pl.multiple_of(source * part, part), part)] = rows.astype(jnp.float32)
    token = whole[...].astype(jnp.bfloat16)
    for copy in copies:
        copy.wait()

    def grouped(rows):
        return jnp.concatenate([rows[:, h * HD : (h + 1) * HD] for h in range(head_count)], axis=0)

    def rounded(weight):
        out = jnp.dot(token, weight[...], preferred_element_type=jnp.float32)
        return out.astype(jnp.bfloat16).astype(jnp.float32)

    new_key = key_of(rounded(forget_w), 1.0 - lower_bound[...])
    query = new_query[...].astype(jnp.float32)
    query = query / (1.0 + jnp.exp(-query))
    reach[...] = grouped(query * (1.0 - new_key))
    key_sum = jnp.sum(grouped(query * new_key), axis=1, keepdims=True)
    addend[...] = key_sum * grouped(rounded(value_w))


def state_kernel(got, reach, final_out, shares, *, axis):
    blocks, _, _ = got.shape
    groups = reach.shape[0]
    row_share = HD // blocks
    head_count, seq_count = final_out.shape[1:3]
    final = [None] * row_share
    later = jnp.zeros((groups, HD), jnp.float32)
    for b in range(blocks - 1, -1, -1):
        tile = got[b, row_share * groups :, :]
        middle, low, power = (
            pltpu.roll(tile, HD - i * row_share, 1) for i in range(1, 4)
        )
        scale = jnp.exp(later) * jnp.exp2(power)
        for d in range(row_share):
            term = scale[:, d : d + 1] * got[b, d * groups : (d + 1) * groups, :]
            final[d] = term if final[d] is None else final[d] + term
        later = later + (tile + (middle + low))
    back = lax.rem(HD - lax.axis_index(axis) * row_share, HD)
    own_reach = pltpu.roll(reach[...], back, 1)
    share = None
    for d in range(row_share):
        for h in range(head_count):
            final_out[d, h] = final[d][h * seq_count : (h + 1) * seq_count].astype(jnp.bfloat16)
        term = own_reach[:, d : d + 1] * final[d]
        share = term if share is None else share + term
    for k in range(blocks):
        shares[k] = share


def read_kernel(shares, addend, read_gain, final, state_cache, first_read):
    state_cache[...] = final[...]
    blocks = shares.shape[0]
    seq_count = first_read.shape[0]
    raw = shares[0]
    for k in range(1, blocks):
        raw = raw + shares[k]
    raw = raw + addend[...]
    mean = jnp.mean(raw * raw, axis=1, keepdims=True)
    normed = raw * lax.rsqrt(mean + 1e-06) * read_gain[...]
    for h in range(first_read.shape[1] // HD):
        first_read[:, h * HD : (h + 1) * HD] = normed[
            h * seq_count : (h + 1) * seq_count
        ].astype(jnp.bfloat16)


def near(array):
    return pltpu.with_memory_space_constraint(array, pltpu.VMEM)


def local(
    prompt, forget_weight, value_weight, lower_bound, extra_decay, new_token, new_query, read_gain
):
    seq_count, span_len, width = prompt.shape
    width_dev = forget_weight.shape[1]
    head_count = width_dev // HD
    blocks = lax.axis_size("sp")
    peers = lax.axis_size("tp")
    row_share = HD // blocks
    groups = head_count * seq_count
    rows = (row_share + 1) * groups
    anywhere = pl.BlockSpec(memory_space=pltpu.HBM)
    vmem = pl.BlockSpec(memory_space=pltpu.VMEM)
    lower_row = lower_bound[None]
    pair = lax.ppermute(new_token, "tp", [(i, i ^ 1) for i in range(peers)])
    sent = pl.pallas_call(
        dense_kernel,
        out_shape=pltpu.VMEM((blocks, rows, HD), jnp.float32),
        in_specs=[anywhere] * 5,
        out_specs=vmem,
        scratch_shapes=[
            pltpu.VMEM((seq_count, span_len, width), jnp.bfloat16),
            pltpu.VMEM((width, width_dev), jnp.bfloat16),
            pltpu.VMEM((width, width_dev), jnp.bfloat16),
            pltpu.VMEM((seq_count, span_len, width_dev), jnp.float32),
            pltpu.VMEM((1, width_dev), jnp.float32),
            pltpu.VMEM((groups, HD), jnp.float32),
            pltpu.SemaphoreType.DMA((3 * PIECES + 2 * (seq_count - 1) + 2,)),
        ],
        name="dense",
    )(prompt, forget_weight, value_weight, lower_row, extra_decay)
    sent = sent.astype(jnp.float16)
    got = lax.all_to_all(sent, "sp", 0, 0, tiled=True)
    token, pair, _ = lax.optimization_barrier((new_token, pair, sent))
    both = jnp.stack([token, pair])
    far = []
    for step in range(1, peers // 2):
        far.append(
            lax.ppermute(both, "tp", [(i, (i + 2 * step) % peers) for i in range(peers)])
        )
    reach, addend = pl.pallas_call(
        functools.partial(token_kernel, axis="tp"),
        out_shape=[pltpu.VMEM((groups, HD), jnp.float32)] * 2,
        in_specs=[vmem] * (2 + len(far)) + [anywhere, anywhere, vmem, vmem],
        out_specs=[vmem] * 2,
        scratch_shapes=[
            pltpu.VMEM((width, width_dev), jnp.bfloat16),
            pltpu.VMEM((width, width_dev), jnp.bfloat16),
            pltpu.VMEM((seq_count, width), jnp.float32),
            pltpu.SemaphoreType.DMA((2,)),
        ],
        name="token",
    )(
        near(token), near(pair), *map(near, far), forget_weight, value_weight,
        near(lower_row), near(new_query),
    )
    got = near(got.astype(jnp.float32))
    final, shares = pl.pallas_call(
        functools.partial(state_kernel, axis="sp"),
        out_shape=[
            pltpu.VMEM((row_share, head_count, seq_count, HD), jnp.bfloat16),
            pltpu.VMEM((blocks, groups, HD), jnp.float32),
        ],
        in_specs=[vmem, vmem],
        out_specs=[vmem, vmem],
        name="state",
    )(got, near(reach))
    shares = near(lax.all_to_all(shares, "sp", 0, 0, tiled=True))
    state_cache, first_read = pl.pallas_call(
        read_kernel,
        out_shape=[
            jax.ShapeDtypeStruct(final.shape, final.dtype),
            jax.ShapeDtypeStruct((seq_count, width_dev), jnp.bfloat16),
        ],
        in_specs=[vmem] * 4,
        out_specs=[vmem] * 2,
        name="read",
    )(shares, near(addend), near(read_gain[None]), near(final))
    return (state_cache, first_read)


def solution(mesh):
    return jax.shard_map(
        local,
        mesh=mesh,
        in_specs=(
            P(None, "sp", None),
            P(None, "tp"),
            P(None, "tp"),
            P("tp"),
            P(None, "sp", "tp"),
            P(None, "tp"),
            P(None, "tp"),
            P(),
        ),
        out_specs=(P("sp", "tp", None, None), P(None, "tp")),
        check_vma=False,
    )
```

```python
import functools

import jax
import jax.numpy as jnp
from jax import lax
from jax.experimental import pallas as pl
from jax.experimental.pallas import tpu as pltpu
from jax.sharding import PartitionSpec as P

HD = 128
PIECES = 4
AHEAD = 5


def log1p_minus(key):
    poly = jnp.float32(1.0 / 7.0)
    for order in range(6, 0, -1):
        poly = poly * key + jnp.float32(1.0 / order)
    return -(key * poly)


def key_of(forget_pre, opening):
    return opening / (1.0 + jnp.exp(forget_pre))


def dense_kernel(
    prompt, forget_weight, value_weight, lower_bound, extra_decay, sent,
    tokens, forget_w, value_w, extra, lower, tot, sems,
):
    seq_count, span_len, width = tokens.shape
    dests = sent.shape[0]
    row_share = HD // dests
    head_count = forget_w.shape[1] // HD
    groups = head_count * seq_count
    piece = width // PIECES
    groups_in = []

    def group(*pairs):
        base = sum(len(copies) for copies in groups_in)
        groups_in.append([
            pltpu.make_async_copy(source, target, sems.at[base + i])
            for i, (source, target) in enumerate(pairs)
        ])

    for p in range(PIECES):
        cut = pl.ds(p * piece, piece)
        group(
            (prompt.at[0, :, cut], tokens.at[0, :, cut]),
            (forget_weight.at[cut], forget_w.at[cut]),
            (value_weight.at[cut], value_w.at[cut]),
        )
    half = span_len // 2
    for s in range(1, seq_count):
        pairs = [
            (prompt.at[s, pl.ds(at, half)], tokens.at[s, pl.ds(at, half)]) for at in (0, half)
        ]
        if s == 1:
            pairs += [(extra_decay, extra), (lower_bound, lower)]
        group(*pairs)

    def start(at):
        if at < len(groups_in):
            for copy in groups_in[at]:
                copy.start()

    def arrive(at):
        for copy in groups_in[at]:
            copy.wait()
        start(at + AHEAD)

    for at in range(AHEAD):
        start(at)

    row = lax.broadcasted_iota(jnp.int32, (span_len, span_len), 0)
    col = lax.broadcasted_iota(jnp.int32, (span_len, span_len), 1)
    after = jnp.where(col > row, 1.0, 0.0).astype(jnp.bfloat16)

    lane = lax.broadcasted_iota(jnp.int32, (HD, HD), 1)
    powers = [jnp.zeros((HD, HD), jnp.float32)]

    def finish(s, opening, forget_pre, values):
        key = key_of(forget_pre.astype(jnp.float32), opening)
        log_forget = log1p_minus(key) + extra[s]
        high = log_forget.astype(jnp.bfloat16)
        left = log_forget - high.astype(jnp.float32)
        middle = left.astype(jnp.bfloat16)
        low = (left - middle.astype(jnp.float32)).astype(jnp.bfloat16)
        later = (
            jnp.dot(after, high, preferred_element_type=jnp.float32)
            + jnp.dot(after, middle, preferred_element_type=jnp.float32)
            + jnp.dot(after, low, preferred_element_type=jnp.float32)
        )
        totals = later[:1] + log_forget[:1]
        weighted = (key * jnp.exp(later)).astype(jnp.bfloat16)
        for h in range(head_count):
            cut = slice(h * HD, (h + 1) * HD)
            group = h * seq_count + s
            tot[group : group + 1, :] = totals[:, cut]
            state = lax.dot_general(
                weighted[:, cut], values[:, cut], (((0,), (0,)), ((), ())),
                preferred_element_type=jnp.float32,
            )
            peak = jnp.max(jnp.abs(state), axis=1, keepdims=True)
            power = jnp.ceil(jnp.log2(jnp.maximum(peak, 1e-30)))
            state = state * jnp.exp2(-power)
            powers[0] = jnp.where(lane == group, power, powers[0])
            for k in range(dests):
                sent[k, pl.ds(group, row_share, stride=groups), :] = state[
                    k * row_share : (k + 1) * row_share
                ]

    forget_sum = value_sum = None
    for p in range(PIECES):
        arrive(p)
        cut = slice(p * piece, (p + 1) * piece)
        part = tokens[0, :, cut]
        forget_part = jnp.dot(part, forget_w[cut], preferred_element_type=jnp.float32)
        value_part = jnp.dot(part, value_w[cut], preferred_element_type=jnp.float32)
        forget_sum = forget_part if p == 0 else forget_sum + forget_part
        value_sum = value_part if p == 0 else value_sum + value_part
    pending = (forget_sum.astype(jnp.bfloat16), value_sum.astype(jnp.bfloat16))
    opening = None
    for s in range(1, seq_count):
        arrive(PIECES + s - 1)
        opening = 1.0 - lower[...]
        forget_pre = jnp.dot(
            tokens[s], forget_w[...], preferred_element_type=jnp.float32
        ).astype(jnp.bfloat16)
        values = jnp.dot(
            tokens[s], value_w[...], preferred_element_type=jnp.float32
        ).astype(jnp.bfloat16)
        finish(s - 1, opening, *pending)
        pending = (forget_pre, values)
    finish(seq_count - 1, opening, *pending)
    total = tot[...]
    high = total.astype(jnp.bfloat16).astype(jnp.float32)
    left = total - high
    middle = left.astype(jnp.bfloat16).astype(jnp.float32)
    parts = (high, middle, left - middle, powers[0].T[:groups])
    at = lax.broadcasted_iota(jnp.int32, (groups, HD), 1) // row_share
    for k in range(dests):
        tile = None
        for i, part in enumerate(parts):
            turned = pltpu.roll(part, (HD + (i - k) * row_share) % HD, 1)
            tile = turned if tile is None else jnp.where(at == i, turned, tile)
        sent[k, row_share * groups :, :] = tile


def chunk_of(weight, chip, step, chips):
    rows = weight.shape[0] // chips
    source = lax.rem(chip + chips - step, chips)
    return weight.at[pl.ds(pl.multiple_of(source * rows, rows), rows)]


def token_start_kernel(
    own, pair, forget_weight, value_weight, sums, forget_w, forget_own, value_own, sems, *, axis
):
    me = lax.axis_index(axis)
    chips = forget_w.shape[0] + 1
    chip = me // 2
    copies = [
        pltpu.make_async_copy(chunk_of(forget_weight, chip, 0, chips), forget_own, sems.at[0]),
        pltpu.make_async_copy(chunk_of(value_weight, chip, 0, chips), value_own, sems.at[1]),
    ]
    for step in range(1, chips):
        copies.append(
            pltpu.make_async_copy(
                chunk_of(forget_weight, chip, step, chips), forget_w.at[step - 1],
                sems.at[step + 1],
            )
        )
    for copy in copies:
        copy.start()
    first, second = own[...].astype(jnp.float32), pair[...].astype(jnp.float32)
    even = lax.rem(me, 2) == 0
    token = jnp.concatenate(
        [jnp.where(even, first, second), jnp.where(even, second, first)], axis=1
    ).astype(jnp.bfloat16)
    for i, weight in enumerate((forget_own, value_own)):
        copies[i].wait()
        sums[i] = jnp.dot(token, weight[...], preferred_element_type=jnp.float32)
    for copy in copies[2:]:
        copy.wait()


def token_kernel(*refs, axis):
    far = refs[:-9]
    sums, forget_w, value_weight, lower_bound, new_query, reach, addend = refs[-9:-2]
    value_w, sems = refs[-2:]
    head_count = forget_w.shape[2] // HD
    me = lax.axis_index(axis)
    chips = forget_w.shape[0] + 1
    copies = [
        pltpu.make_async_copy(
            chunk_of(value_weight, me // 2, step, chips), value_w.at[step - 1], sems.at[step - 1]
        )
        for step in range(1, chips)
    ]
    for copy in copies:
        copy.start()
    even = lax.rem(me, 2) == 0
    tokens = []
    for pieces in far:
        first, second = (pieces[i].astype(jnp.float32) for i in (0, 1))
        tokens += [jnp.where(even, first, second), jnp.where(even, second, first)]
    token = jnp.concatenate(tokens, axis=1).astype(jnp.bfloat16)

    def grouped(rows):
        return jnp.concatenate([rows[:, h * HD : (h + 1) * HD] for h in range(head_count)], axis=0)

    def rounded(i, weight):
        weight = weight[...].reshape(token.shape[1], weight.shape[2])
        out = sums[i] + jnp.dot(token, weight, preferred_element_type=jnp.float32)
        return out.astype(jnp.bfloat16).astype(jnp.float32)

    new_key = key_of(rounded(0, forget_w), 1.0 - lower_bound[...])
    query = new_query[...].astype(jnp.float32)
    query = query / (1.0 + jnp.exp(-query))
    reach[...] = grouped(query * (1.0 - new_key))
    key_sum = jnp.sum(grouped(query * new_key), axis=1, keepdims=True)
    for copy in copies:
        copy.wait()
    addend[...] = key_sum * grouped(rounded(1, value_w))


def state_kernel(got, reach, final_out, shares, *, axis):
    blocks, _, _ = got.shape
    groups = reach.shape[0]
    row_share = HD // blocks
    head_count, seq_count = final_out.shape[1:3]
    final = [None] * row_share
    later = jnp.zeros((groups, HD), jnp.float32)
    for b in range(blocks - 1, -1, -1):
        tile = got[b, row_share * groups :, :]
        middle, low, power = (
            pltpu.roll(tile, HD - i * row_share, 1) for i in range(1, 4)
        )
        scale = jnp.exp(later) * jnp.exp2(power)
        for d in range(row_share):
            term = scale[:, d : d + 1] * got[b, d * groups : (d + 1) * groups, :]
            final[d] = term if final[d] is None else final[d] + term
        later = later + (tile + (middle + low))
    back = lax.rem(HD - lax.axis_index(axis) * row_share, HD)
    own_reach = pltpu.roll(reach[...], back, 1)
    share = None
    for d in range(row_share):
        for h in range(head_count):
            final_out[d, h] = final[d][h * seq_count : (h + 1) * seq_count].astype(jnp.bfloat16)
        term = own_reach[:, d : d + 1] * final[d]
        share = term if share is None else share + term
    for k in range(blocks):
        shares[k] = share


def read_kernel(shares, addend, read_gain, final, state_cache, first_read):
    state_cache[...] = final[...]
    blocks = shares.shape[0]
    seq_count = first_read.shape[0]
    raw = shares[0]
    for k in range(1, blocks):
        raw = raw + shares[k]
    raw = raw + addend[...]
    mean = jnp.mean(raw * raw, axis=1, keepdims=True)
    normed = raw * lax.rsqrt(mean + 1e-06) * read_gain[...]
    for h in range(first_read.shape[1] // HD):
        first_read[:, h * HD : (h + 1) * HD] = normed[
            h * seq_count : (h + 1) * seq_count
        ].astype(jnp.bfloat16)


def near(array):
    return pltpu.with_memory_space_constraint(array, pltpu.VMEM)


def local(
    prompt, forget_weight, value_weight, lower_bound, extra_decay, new_token, new_query, read_gain
):
    seq_count, span_len, width = prompt.shape
    width_dev = forget_weight.shape[1]
    head_count = width_dev // HD
    blocks = lax.axis_size("sp")
    peers = lax.axis_size("tp")
    row_share = HD // blocks
    groups = head_count * seq_count
    rows = (row_share + 1) * groups
    anywhere = pl.BlockSpec(memory_space=pltpu.HBM)
    vmem = pl.BlockSpec(memory_space=pltpu.VMEM)
    lower_row = lower_bound[None]
    pair = lax.ppermute(new_token, "tp", [(i, i ^ 1) for i in range(peers)])
    sent = pl.pallas_call(
        dense_kernel,
        out_shape=pltpu.VMEM((blocks, rows, HD), jnp.float32),
        in_specs=[anywhere] * 5,
        out_specs=vmem,
        scratch_shapes=[
            pltpu.VMEM((seq_count, span_len, width), jnp.bfloat16),
            pltpu.VMEM((width, width_dev), jnp.bfloat16),
            pltpu.VMEM((width, width_dev), jnp.bfloat16),
            pltpu.VMEM((seq_count, span_len, width_dev), jnp.float32),
            pltpu.VMEM((1, width_dev), jnp.float32),
            pltpu.VMEM((groups, HD), jnp.float32),
            pltpu.SemaphoreType.DMA((3 * PIECES + 2 * (seq_count - 1) + 2,)),
        ],
        name="dense",
    )(prompt, forget_weight, value_weight, lower_row, extra_decay)
    sent = sent.astype(jnp.float16)
    got = lax.all_to_all(sent, "sp", 0, 0, tiled=True)
    token, pair, _ = lax.optimization_barrier((new_token, pair, sent))
    both = jnp.stack([token, pair])
    far = []
    for step in range(1, peers // 2):
        far.append(lax.ppermute(both, "tp", [(i, (i + 2 * step) % peers) for i in range(peers)]))
    others = len(far)
    part = width // (others + 1)
    sums, forget_far = pl.pallas_call(
        functools.partial(token_start_kernel, axis="tp"),
        out_shape=[
            pltpu.VMEM((2, seq_count, width_dev), jnp.float32),
            pltpu.VMEM((others, part, width_dev), jnp.bfloat16),
        ],
        in_specs=[vmem, vmem, anywhere, anywhere],
        out_specs=[vmem] * 2,
        scratch_shapes=[
            pltpu.VMEM((part, width_dev), jnp.bfloat16),
            pltpu.VMEM((part, width_dev), jnp.bfloat16),
            pltpu.SemaphoreType.DMA((others + 2,)),
        ],
        name="prepare",
    )(near(token), near(pair), forget_weight, value_weight)
    reach, addend = pl.pallas_call(
        functools.partial(token_kernel, axis="tp"),
        out_shape=[pltpu.VMEM((groups, HD), jnp.float32)] * 2,
        in_specs=[vmem] * (others + 2) + [anywhere, vmem, vmem],
        out_specs=[vmem] * 2,
        scratch_shapes=[
            pltpu.VMEM((others, part, width_dev), jnp.bfloat16),
            pltpu.SemaphoreType.DMA((others,)),
        ],
        name="token",
    )(
        *map(near, far), near(sums), near(forget_far), value_weight, near(lower_row),
        near(new_query),
    )
    got = near(got.astype(jnp.float32))
    final, shares = pl.pallas_call(
        functools.partial(state_kernel, axis="sp"),
        out_shape=[
            pltpu.VMEM((row_share, head_count, seq_count, HD), jnp.bfloat16),
            pltpu.VMEM((blocks, groups, HD), jnp.float32),
        ],
        in_specs=[vmem, vmem],
        out_specs=[vmem, vmem],
        name="state",
    )(got, near(reach))
    shares = near(lax.all_to_all(shares, "sp", 0, 0, tiled=True))
    state_cache, first_read = pl.pallas_call(
        read_kernel,
        out_shape=[
            jax.ShapeDtypeStruct(final.shape, final.dtype),
            jax.ShapeDtypeStruct((seq_count, width_dev), jnp.bfloat16),
        ],
        in_specs=[vmem] * 4,
        out_specs=[vmem] * 2,
        name="read",
    )(shares, near(addend), near(read_gain[None]), near(final))
    return (state_cache, first_read)


def solution(mesh):
    return jax.shard_map(
        local,
        mesh=mesh,
        in_specs=(
            P(None, "sp", None),
            P(None, "tp"),
            P(None, "tp"),
            P("tp"),
            P(None, "sp", "tp"),
            P(None, "tp"),
            P(None, "tp"),
            P(),
        ),
        out_specs=(P("sp", "tp", None, None), P(None, "tp")),
        check_vma=False,
    )
```

```python
import functools

import jax
import jax.numpy as jnp
from jax import lax
from jax.experimental import pallas as pl
from jax.experimental.pallas import tpu as pltpu
from jax.sharding import PartitionSpec as P

HD = 128
TILE = 8
PIECES = 4
AHEAD = 5


def log1p_minus(key):
    poly = jnp.float32(1.0 / 7.0)
    for order in range(6, 0, -1):
        poly = poly * key + jnp.float32(1.0 / order)
    return -(key * poly)


def key_of(forget_pre, opening):
    return opening / (1.0 + jnp.exp(forget_pre))


def side_by_side(parts):
    size = HD // len(parts)
    out = parts[0]
    if len(parts) > 1:
        shape = jnp.broadcast_shapes(*(part.shape for part in parts))
        lane = lax.broadcasted_iota(jnp.int32, (*shape[:-1], HD), len(shape) - 1)
        for g in range(1, len(parts)):
            out = jnp.where(lane >= g * size, parts[g], out)
    return out


def dense_kernel(
    prompt, forget_weight, value_weight, lower_bound, extra_decay, sent,
    tokens, forget_w, value_w, extra, lower, tot, sems,
):
    seq_count, span_len, width = tokens.shape
    dests = sent.shape[0]
    head_count = forget_w.shape[1] // HD
    groups = head_count * seq_count
    per = dests // groups
    size = HD // per
    piece = width // PIECES
    groups_in = []

    def group(*pairs):
        base = sum(len(copies) for copies in groups_in)
        groups_in.append([
            pltpu.make_async_copy(source, target, sems.at[base + i])
            for i, (source, target) in enumerate(pairs)
        ])

    for p in range(PIECES):
        cut = pl.ds(p * piece, piece)
        group(
            (prompt.at[0, :, cut], tokens.at[0, :, cut]),
            (forget_weight.at[cut], forget_w.at[cut]),
            (value_weight.at[cut], value_w.at[cut]),
        )
    half = span_len // 2
    for s in range(1, seq_count):
        pairs = [
            (prompt.at[s, pl.ds(at, half)], tokens.at[s, pl.ds(at, half)]) for at in (0, half)
        ]
        if s == 1:
            pairs += [(extra_decay, extra), (lower_bound, lower)]
        group(*pairs)

    def start(at):
        if at < len(groups_in):
            for copy in groups_in[at]:
                copy.start()

    def arrive(at):
        for copy in groups_in[at]:
            copy.wait()
        start(at + AHEAD)

    for at in range(AHEAD):
        start(at)


    lane = lax.broadcasted_iota(jnp.int32, (HD, HD), 1)
    powers = [jnp.zeros((HD, HD), jnp.float32)]

    def finish(s, opening, forget_pre, values):
        key = key_of(forget_pre.astype(jnp.float32), opening)
        log_forget = log1p_minus(key) + extra[s]
        tiles = log_forget.reshape(span_len // TILE, TILE, -1)
        sub = lax.broadcasted_iota(jnp.int32, tiles.shape, 1)
        inside = jnp.where(sub < TILE - 1, pltpu.roll(tiles, TILE - 1, 1), 0.0)
        step = 1
        while step < TILE:
            inside = inside + jnp.where(sub < TILE - step, pltpu.roll(inside, TILE - step, 1), 0.0)
            step *= 2
        carry = jnp.zeros((1, log_forget.shape[1]), jnp.float32)
        beyond = []
        for at in range(span_len // TILE - 1, -1, -1):
            beyond.append(inside[at] + carry)
            carry = carry + (inside[at, :1] + tiles[at, :1])
        later = jnp.concatenate(beyond[::-1], axis=0)
        totals = carry
        weighted = (key * jnp.exp(later)).astype(jnp.bfloat16)
        for h in range(head_count):
            cut = slice(h * HD, (h + 1) * HD)
            group = h * seq_count + s
            tot[group : group + 1, :] = totals[:, cut]
            state = lax.dot_general(
                weighted[:, cut], values[:, cut], (((0,), (0,)), ((), ())),
                preferred_element_type=jnp.float32,
            )
            peak = jnp.max(jnp.abs(state), axis=1, keepdims=True)
            power = jnp.ceil(jnp.log2(jnp.maximum(peak, 1e-30)))
            state = state * jnp.exp2(-power)
            powers[0] = jnp.where(lane == group, power, powers[0])
            for c in range(per):
                turned = [
                    pltpu.roll(state[g * size : (g + 1) * size], (g - c) * size % HD, 1)
                    if g != c
                    else state[g * size : (g + 1) * size]
                    for g in range(per)
                ]
                sent[group * per + c, :size, :] = side_by_side(turned)

    forget_sum = value_sum = None
    for p in range(PIECES):
        arrive(p)
        cut = slice(p * piece, (p + 1) * piece)
        part = tokens[0, :, cut]
        forget_part = jnp.dot(part, forget_w[cut], preferred_element_type=jnp.float32)
        value_part = jnp.dot(part, value_w[cut], preferred_element_type=jnp.float32)
        forget_sum = forget_part if p == 0 else forget_sum + forget_part
        value_sum = value_part if p == 0 else value_sum + value_part
    pending = (forget_sum.astype(jnp.bfloat16), value_sum.astype(jnp.bfloat16))
    opening = None
    for s in range(1, seq_count):
        arrive(PIECES + s - 1)
        opening = 1.0 - lower[...]
        finish(s - 1, opening, *pending)
        forget_pre = jnp.dot(
            tokens[s], forget_w[...], preferred_element_type=jnp.float32
        ).astype(jnp.bfloat16)
        values = jnp.dot(
            tokens[s], value_w[...], preferred_element_type=jnp.float32
        ).astype(jnp.bfloat16)
        pending = (forget_pre, values)
    finish(seq_count - 1, opening, *pending)
    total = tot[...]
    high = total.astype(jnp.bfloat16).astype(jnp.float32)
    left = total - high
    middle = left.astype(jnp.bfloat16).astype(jnp.float32)
    parts = (powers[0].T[:groups], high, middle, left - middle)
    for k in range(dests):
        group = k // per
        for i, part in enumerate(parts):
            sent[k, size + i : size + i + 1, :] = part[group : group + 1]


def chunk_of(weight, chip, step, chips):
    rows = weight.shape[0] // chips
    source = lax.rem(chip + chips - step, chips)
    return weight.at[pl.ds(pl.multiple_of(source * rows, rows), rows)]


def token_start_kernel(
    own, pair, forget_weight, value_weight, sums, forget_w, forget_own, value_own, sems, *, axis
):
    me = lax.axis_index(axis)
    chips = forget_w.shape[0] + 1
    chip = me // 2
    copies = [
        pltpu.make_async_copy(chunk_of(forget_weight, chip, 0, chips), forget_own, sems.at[0]),
        pltpu.make_async_copy(chunk_of(value_weight, chip, 0, chips), value_own, sems.at[1]),
    ]
    for step in range(1, chips):
        copies.append(
            pltpu.make_async_copy(
                chunk_of(forget_weight, chip, step, chips), forget_w.at[step - 1],
                sems.at[step + 1],
            )
        )
    for copy in copies:
        copy.start()
    first, second = own[...].astype(jnp.float32), pair[...].astype(jnp.float32)
    even = lax.rem(me, 2) == 0
    token = jnp.concatenate(
        [jnp.where(even, first, second), jnp.where(even, second, first)], axis=1
    ).astype(jnp.bfloat16)
    for i, weight in enumerate((forget_own, value_own)):
        copies[i].wait()
        sums[i] = jnp.dot(token, weight[...], preferred_element_type=jnp.float32)
    for copy in copies[2:]:
        copy.wait()


def token_kernel(*refs, axis):
    far = refs[:-9]
    sums, forget_w, value_weight, lower_bound, new_query, reach, addend = refs[-9:-2]
    value_w, sems = refs[-2:]
    head_count = forget_w.shape[2] // HD
    me = lax.axis_index(axis)
    chips = forget_w.shape[0] + 1
    copies = [
        pltpu.make_async_copy(
            chunk_of(value_weight, me // 2, step, chips), value_w.at[step - 1], sems.at[step - 1]
        )
        for step in range(1, chips)
    ]
    for copy in copies:
        copy.start()
    even = lax.rem(me, 2) == 0
    tokens = []
    for pieces in far:
        first, second = (pieces[i].astype(jnp.float32) for i in (0, 1))
        tokens += [jnp.where(even, first, second), jnp.where(even, second, first)]
    token = jnp.concatenate(tokens, axis=1).astype(jnp.bfloat16)

    def grouped(rows):
        return jnp.concatenate([rows[:, h * HD : (h + 1) * HD] for h in range(head_count)], axis=0)

    def rounded(i, weight):
        weight = weight[...].reshape(token.shape[1], weight.shape[2])
        out = sums[i] + jnp.dot(token, weight, preferred_element_type=jnp.float32)
        return out.astype(jnp.bfloat16).astype(jnp.float32)

    new_key = key_of(rounded(0, forget_w), 1.0 - lower_bound[...])
    query = new_query[...].astype(jnp.float32)
    query = query / (1.0 + jnp.exp(-query))
    reach[...] = grouped(query * (1.0 - new_key))
    key_sum = jnp.sum(grouped(query * new_key), axis=1, keepdims=True)
    for copy in copies:
        copy.wait()
    addend[...] = key_sum * grouped(rounded(1, value_w))


def state_kernel(got, reach, shares, scales, powers, *, axis):
    blocks, _, _ = got.shape
    groups = reach.shape[0]
    per = blocks // groups
    size = HD // per
    row_share = HD // blocks
    later = jnp.zeros((1, HD), jnp.float32)
    for b in range(blocks - 1, -1, -1):
        scales[b : b + 1, :] = later
        powers[b : b + 1, :] = got[b, size : size + 1, :]
        later = later + (
            got[b, size + 1 : size + 2, :]
            + (got[b, size + 2 : size + 3, :] + got[b, size + 3 : size + 4, :])
        )
    scales[:blocks] = jnp.exp(scales[:blocks]) * jnp.exp2(powers[...])
    group = lax.axis_index(axis) // per
    scales[blocks : blocks + 1, :] = reach[pl.ds(group, 1), :]
    by_key = scales[...].T

    def spread(column):
        return side_by_side(
            [
                jnp.broadcast_to(by_key[g * size : (g + 1) * size, column : column + 1], (size, HD))
                for g in range(per)
            ]
        )

    final = None
    for b in range(blocks):
        term = spread(b) * got[b, :size, :]
        final = term if final is None else final + term
    read = jnp.sum(spread(blocks) * final, axis=0, keepdims=True)
    step = HD // 2
    while step >= size:
        read = read + pltpu.roll(jnp.broadcast_to(read, (8, HD)), step, 1)[:1]
        step //= 2
    lane = lax.broadcasted_iota(jnp.int32, (size, HD), 1)
    for g in range(per):
        turned = final if g == 0 else pltpu.roll(final, HD - g * size, 1)
        turned = jnp.where(lane < size, turned, jnp.broadcast_to(read, (size, HD)))
        for m in range(size // row_share):
            shares[g * (size // row_share) + m] = turned[m * row_share : (m + 1) * row_share]


def read_kernel(shares, addend, read_gain, state_cache, first_read, held):
    row_share, head_count, seq_count, _ = state_cache.shape
    groups = head_count * seq_count
    per, _, _ = held.shape
    size = HD // per
    for group in range(groups):
        for c in range(per):
            held[c, pl.ds(group, row_share, stride=groups), :] = shares[group * per + c]
    final = side_by_side(
        [held[c] if c == 0 else pltpu.roll(held[c], c * size, 1) for c in range(per)]
    )
    for d in range(row_share):
        for h in range(head_count):
            at = d * groups + h * seq_count
            state_cache[d, h] = final[at : at + seq_count].astype(jnp.bfloat16)
    raw = side_by_side(
        [
            held[c, :groups] if c == 1 else pltpu.roll(held[c, :groups], (c - 1) * size % HD, 1)
            for c in range(per)
        ]
    )
    raw = raw + addend[...]
    mean = jnp.mean(raw * raw, axis=1, keepdims=True)
    normed = raw * lax.rsqrt(mean + 1e-06) * read_gain[...]
    for h in range(head_count):
        first_read[:, h * HD : (h + 1) * HD] = normed[
            h * seq_count : (h + 1) * seq_count
        ].astype(jnp.bfloat16)


def near(array):
    return pltpu.with_memory_space_constraint(array, pltpu.VMEM)


def local(
    prompt, forget_weight, value_weight, lower_bound, extra_decay, new_token, new_query, read_gain
):
    seq_count, span_len, width = prompt.shape
    width_dev = forget_weight.shape[1]
    head_count = width_dev // HD
    blocks = lax.axis_size("sp")
    peers = lax.axis_size("tp")
    row_share = HD // blocks
    groups = head_count * seq_count
    rows = HD // (blocks // groups) + 8
    anywhere = pl.BlockSpec(memory_space=pltpu.HBM)
    vmem = pl.BlockSpec(memory_space=pltpu.VMEM)
    lower_row = lower_bound[None]
    pair = lax.ppermute(new_token, "tp", [(i, i ^ 1) for i in range(peers)])
    sent = pl.pallas_call(
        dense_kernel,
        out_shape=pltpu.VMEM((blocks, rows, HD), jnp.float32),
        in_specs=[anywhere] * 5,
        out_specs=vmem,
        scratch_shapes=[
            pltpu.VMEM((seq_count, span_len, width), jnp.bfloat16),
            pltpu.VMEM((width, width_dev), jnp.bfloat16),
            pltpu.VMEM((width, width_dev), jnp.bfloat16),
            pltpu.VMEM((seq_count, span_len, width_dev), jnp.float32),
            pltpu.VMEM((1, width_dev), jnp.float32),
            pltpu.VMEM((groups, HD), jnp.float32),
            pltpu.SemaphoreType.DMA((3 * PIECES + 2 * (seq_count - 1) + 2,)),
        ],
        name="dense",
    )(prompt, forget_weight, value_weight, lower_row, extra_decay)
    sent = sent.astype(jnp.float16)
    got = lax.all_to_all(sent, "sp", 0, 0, tiled=True)
    token, pair, _ = lax.optimization_barrier((new_token, pair, sent))
    both = jnp.stack([token, pair])
    far = []
    for step in range(1, peers // 2):
        far.append(lax.ppermute(both, "tp", [(i, (i + 2 * step) % peers) for i in range(peers)]))
    others = len(far)
    part = width // (others + 1)
    sums, forget_far = pl.pallas_call(
        functools.partial(token_start_kernel, axis="tp"),
        out_shape=[
            pltpu.VMEM((2, seq_count, width_dev), jnp.float32),
            pltpu.VMEM((others, part, width_dev), jnp.bfloat16),
        ],
        in_specs=[vmem, vmem, anywhere, anywhere],
        out_specs=[vmem] * 2,
        scratch_shapes=[
            pltpu.VMEM((part, width_dev), jnp.bfloat16),
            pltpu.VMEM((part, width_dev), jnp.bfloat16),
            pltpu.SemaphoreType.DMA((others + 2,)),
        ],
        name="prepare",
    )(near(token), near(pair), forget_weight, value_weight)
    reach, addend = pl.pallas_call(
        functools.partial(token_kernel, axis="tp"),
        out_shape=[pltpu.VMEM((groups, HD), jnp.float32)] * 2,
        in_specs=[vmem] * (others + 2) + [anywhere, vmem, vmem],
        out_specs=[vmem] * 2,
        scratch_shapes=[
            pltpu.VMEM((others, part, width_dev), jnp.bfloat16),
            pltpu.SemaphoreType.DMA((others,)),
        ],
        name="token",
    )(
        *map(near, far), near(sums), near(forget_far), value_weight, near(lower_row),
        near(new_query),
    )
    got = near(got.astype(jnp.float32))
    shares = pl.pallas_call(
        functools.partial(state_kernel, axis="sp"),
        out_shape=pltpu.VMEM((blocks, row_share, HD), jnp.float32),
        in_specs=[vmem, vmem],
        out_specs=vmem,
        scratch_shapes=[
            pltpu.VMEM((HD, HD), jnp.float32),
            pltpu.VMEM((blocks, HD), jnp.float32),
        ],
        name="state",
    )(got, near(reach))
    shares = near(lax.all_to_all(shares, "sp", 0, 0, tiled=True))
    state_cache, first_read = pl.pallas_call(
        read_kernel,
        out_shape=[
            jax.ShapeDtypeStruct((row_share, head_count, seq_count, HD), jnp.bfloat16),
            jax.ShapeDtypeStruct((seq_count, width_dev), jnp.bfloat16),
        ],
        in_specs=[vmem] * 3,
        out_specs=[vmem] * 2,
        scratch_shapes=[pltpu.VMEM((blocks // groups, row_share * groups, HD), jnp.float32)],
        name="read",
    )(shares, near(addend), near(read_gain[None]))
    return (state_cache, first_read)


def solution(mesh):
    return jax.shard_map(
        local,
        mesh=mesh,
        in_specs=(
            P(None, "sp", None),
            P(None, "tp"),
            P(None, "tp"),
            P("tp"),
            P(None, "sp", "tp"),
            P(None, "tp"),
            P(None, "tp"),
            P(),
        ),
        out_specs=(P("sp", "tp", None, None), P(None, "tp")),
        check_vma=False,
    )
```

```python
import functools

import jax
import jax.numpy as jnp
from jax import lax
from jax.experimental import pallas as pl
from jax.experimental.pallas import tpu as pltpu
from jax.sharding import PartitionSpec as P

HD = 128
TILE = 8
PIECES = 4
AHEAD = 7


def log1p_minus(key):
    poly = jnp.float32(1.0 / 7.0)
    for order in range(6, 0, -1):
        poly = poly * key + jnp.float32(1.0 / order)
    return -(key * poly)


def key_of(forget_pre, opening):
    return opening / (1.0 + jnp.exp(forget_pre))


def side_by_side(parts):
    size = HD // len(parts)
    out = parts[0]
    if len(parts) > 1:
        shape = jnp.broadcast_shapes(*(part.shape for part in parts))
        lane = lax.broadcasted_iota(jnp.int32, (*shape[:-1], HD), len(shape) - 1)
        for g in range(1, len(parts)):
            out = jnp.where(lane >= g * size, parts[g], out)
    return out


def dense_kernel(
    prompt, forget_weight, value_weight, lower_bound, extra_decay, sent,
    tokens, forget_w, value_w, extra, lower, tot, sems,
):
    seq_count, span_len, width = tokens.shape
    dests = sent.shape[0]
    head_count = forget_w.shape[1] // HD
    groups = head_count * seq_count
    per = dests // groups
    size = HD // per
    piece = width // PIECES
    groups_in = []

    def group(*pairs):
        base = sum(len(copies) for copies in groups_in)
        groups_in.append([
            pltpu.make_async_copy(source, target, sems.at[base + i])
            for i, (source, target) in enumerate(pairs)
        ])

    for p in range(PIECES):
        cut = pl.ds(p * piece, piece)
        group(
            (prompt.at[0, :, cut], tokens.at[0, :, cut]),
            (forget_weight.at[cut], forget_w.at[cut]),
            (value_weight.at[cut], value_w.at[cut]),
        )
    half = span_len // 2
    for s in range(1, seq_count):
        pairs = [
            (prompt.at[s, pl.ds(at, half)], tokens.at[s, pl.ds(at, half)]) for at in (0, half)
        ]
        if s == 1:
            pairs += [(extra_decay, extra), (lower_bound, lower)]
        group(*pairs)

    def start(at):
        if at < len(groups_in):
            for copy in groups_in[at]:
                copy.start()

    def arrive(at):
        for copy in groups_in[at]:
            copy.wait()
        start(at + AHEAD)

    for at in range(AHEAD):
        start(at)


    lane = lax.broadcasted_iota(jnp.int32, (HD, HD), 1)
    powers = [jnp.zeros((HD, HD), jnp.float32)]

    def finish(s, opening, forget_pre, values):
        key = key_of(forget_pre.astype(jnp.float32), opening)
        log_forget = log1p_minus(key) + extra[s]
        tiles = log_forget.reshape(span_len // TILE, TILE, -1)
        sub = lax.broadcasted_iota(jnp.int32, tiles.shape, 1)
        inside = jnp.where(sub < TILE - 1, pltpu.roll(tiles, TILE - 1, 1), 0.0)
        step = 1
        while step < TILE:
            inside = inside + jnp.where(sub < TILE - step, pltpu.roll(inside, TILE - step, 1), 0.0)
            step *= 2
        carry = jnp.zeros((1, log_forget.shape[1]), jnp.float32)
        beyond = []
        for at in range(span_len // TILE - 1, -1, -1):
            beyond.append(inside[at] + carry)
            carry = carry + (inside[at, :1] + tiles[at, :1])
        later = jnp.concatenate(beyond[::-1], axis=0)
        totals = carry
        weighted = (key * jnp.exp(later)).astype(jnp.bfloat16)
        for h in range(head_count):
            cut = slice(h * HD, (h + 1) * HD)
            group = h * seq_count + s
            tot[group : group + 1, :] = totals[:, cut]
            state = lax.dot_general(
                weighted[:, cut], values[:, cut], (((0,), (0,)), ((), ())),
                preferred_element_type=jnp.float32,
            )
            peak = jnp.max(jnp.abs(state), axis=1, keepdims=True)
            power = jnp.ceil(jnp.log2(jnp.maximum(peak, 1e-30)))
            state = state * jnp.exp2(-power)
            powers[0] = jnp.where(lane == group, power, powers[0])
            for c in range(per):
                turned = [
                    pltpu.roll(state[g * size : (g + 1) * size], (g - c) * size % HD, 1)
                    if g != c
                    else state[g * size : (g + 1) * size]
                    for g in range(per)
                ]
                sent[group * per + c, :size, :] = side_by_side(turned)

    forget_sum = value_sum = None
    for p in range(PIECES):
        arrive(p)
        cut = slice(p * piece, (p + 1) * piece)
        part = tokens[0, :, cut]
        forget_part = jnp.dot(part, forget_w[cut], preferred_element_type=jnp.float32)
        value_part = jnp.dot(part, value_w[cut], preferred_element_type=jnp.float32)
        forget_sum = forget_part if p == 0 else forget_sum + forget_part
        value_sum = value_part if p == 0 else value_sum + value_part
    pending = (forget_sum.astype(jnp.bfloat16), value_sum.astype(jnp.bfloat16))
    opening = None
    for s in range(1, seq_count):
        arrive(PIECES + s - 1)
        opening = 1.0 - lower[...]
        finish(s - 1, opening, *pending)
        forget_pre = jnp.dot(
            tokens[s], forget_w[...], preferred_element_type=jnp.float32
        ).astype(jnp.bfloat16)
        values = jnp.dot(
            tokens[s], value_w[...], preferred_element_type=jnp.float32
        ).astype(jnp.bfloat16)
        pending = (forget_pre, values)
    finish(seq_count - 1, opening, *pending)
    total = tot[...]
    high = total.astype(jnp.bfloat16).astype(jnp.float32)
    left = total - high
    middle = left.astype(jnp.bfloat16).astype(jnp.float32)
    parts = (powers[0].T[:groups], high, middle, left - middle)
    for k in range(dests):
        group = k // per
        for i, part in enumerate(parts):
            sent[k, size + i : size + i + 1, :] = part[group : group + 1]


def chunk_of(weight, chip, step, chips):
    rows = weight.shape[0] // chips
    source = lax.rem(chip + chips - step, chips)
    return weight.at[pl.ds(pl.multiple_of(source * rows, rows), rows)]


def token_start_kernel(
    own, pair, forget_weight, value_weight, sums, forget_w, forget_own, value_own, sems, *, axis
):
    me = lax.axis_index(axis)
    chips = forget_w.shape[0] + 1
    chip = me // 2
    copies = [
        pltpu.make_async_copy(chunk_of(forget_weight, chip, 0, chips), forget_own, sems.at[0]),
        pltpu.make_async_copy(chunk_of(value_weight, chip, 0, chips), value_own, sems.at[1]),
    ]
    for step in range(1, chips):
        copies.append(
            pltpu.make_async_copy(
                chunk_of(forget_weight, chip, step, chips), forget_w.at[step - 1],
                sems.at[step + 1],
            )
        )
    for copy in copies:
        copy.start()
    first, second = own[...].astype(jnp.float32), pair[...].astype(jnp.float32)
    even = lax.rem(me, 2) == 0
    token = jnp.concatenate(
        [jnp.where(even, first, second), jnp.where(even, second, first)], axis=1
    ).astype(jnp.bfloat16)
    for i, weight in enumerate((forget_own, value_own)):
        copies[i].wait()
        sums[i] = jnp.dot(token, weight[...], preferred_element_type=jnp.float32)
    for copy in copies[2:]:
        copy.wait()


def token_kernel(*refs, axis):
    far = refs[:-9]
    sums, forget_w, value_weight, lower_bound, new_query, reach, addend = refs[-9:-2]
    value_w, sems = refs[-2:]
    head_count = forget_w.shape[2] // HD
    me = lax.axis_index(axis)
    chips = forget_w.shape[0] + 1
    copies = [
        pltpu.make_async_copy(
            chunk_of(value_weight, me // 2, step, chips), value_w.at[step - 1], sems.at[step - 1]
        )
        for step in range(1, chips)
    ]
    for copy in copies:
        copy.start()
    even = lax.rem(me, 2) == 0
    tokens = []
    for pieces in far:
        first, second = (pieces[i].astype(jnp.float32) for i in (0, 1))
        tokens += [jnp.where(even, first, second), jnp.where(even, second, first)]
    token = jnp.concatenate(tokens, axis=1).astype(jnp.bfloat16)

    def grouped(rows):
        return jnp.concatenate([rows[:, h * HD : (h + 1) * HD] for h in range(head_count)], axis=0)

    def rounded(i, weight):
        weight = weight[...].reshape(token.shape[1], weight.shape[2])
        out = sums[i] + jnp.dot(token, weight, preferred_element_type=jnp.float32)
        return out.astype(jnp.bfloat16).astype(jnp.float32)

    new_key = key_of(rounded(0, forget_w), 1.0 - lower_bound[...])
    query = new_query[...].astype(jnp.float32)
    query = query / (1.0 + jnp.exp(-query))
    reach[...] = grouped(query * (1.0 - new_key))
    key_sum = jnp.sum(grouped(query * new_key), axis=1, keepdims=True)
    for copy in copies:
        copy.wait()
    addend[...] = key_sum * grouped(rounded(1, value_w))


def state_kernel(got, reach, shares, scales, powers, *, axis):
    blocks, _, _ = got.shape
    groups = reach.shape[0]
    per = blocks // groups
    size = HD // per
    row_share = HD // blocks
    later = jnp.zeros((1, HD), jnp.float32)
    for b in range(blocks - 1, -1, -1):
        scales[b : b + 1, :] = later
        powers[b : b + 1, :] = got[b, size : size + 1, :]
        later = later + (
            got[b, size + 1 : size + 2, :]
            + (got[b, size + 2 : size + 3, :] + got[b, size + 3 : size + 4, :])
        )
    scales[:blocks] = jnp.exp(scales[:blocks]) * jnp.exp2(powers[...])
    group = lax.axis_index(axis) // per
    scales[blocks : blocks + 1, :] = reach[pl.ds(group, 1), :]
    by_key = scales[...].T

    def spread(column):
        return side_by_side(
            [
                jnp.broadcast_to(by_key[g * size : (g + 1) * size, column : column + 1], (size, HD))
                for g in range(per)
            ]
        )

    final = None
    for b in range(blocks):
        term = spread(b) * got[b, :size, :]
        final = term if final is None else final + term
    read = jnp.sum(spread(blocks) * final, axis=0, keepdims=True)
    step = HD // 2
    while step >= size:
        read = read + pltpu.roll(jnp.broadcast_to(read, (8, HD)), step, 1)[:1]
        step //= 2
    lane = lax.broadcasted_iota(jnp.int32, (size, HD), 1)
    for g in range(per):
        turned = final if g == 0 else pltpu.roll(final, HD - g * size, 1)
        turned = jnp.where(lane < size, turned, jnp.broadcast_to(read, (size, HD)))
        for m in range(size // row_share):
            shares[g * (size // row_share) + m] = turned[m * row_share : (m + 1) * row_share]


def read_kernel(shares, addend, read_gain, state_cache, first_read, held):
    row_share, head_count, seq_count, _ = state_cache.shape
    groups = head_count * seq_count
    per = shares.shape[0] // groups
    size = HD // per
    for group in range(groups):
        for c in range(per):
            held[c, pl.ds(group, row_share, stride=groups), :] = shares[group * per + c]
    final = side_by_side(
        [held[c] if c == 0 else pltpu.roll(held[c], c * size, 1) for c in range(per)]
    )
    for d in range(row_share):
        for h in range(head_count):
            at = d * groups + h * seq_count
            state_cache[d, h] = final[at : at + seq_count].astype(jnp.bfloat16)
    raw = side_by_side(
        [
            held[c, :groups] if c == 1 else pltpu.roll(held[c, :groups], (c - 1) * size % HD, 1)
            for c in range(per)
        ]
    )
    raw = raw + addend[...]
    mean = jnp.mean(raw * raw, axis=1, keepdims=True)
    normed = raw * lax.rsqrt(mean + 1e-06) * read_gain[...]
    for h in range(head_count):
        first_read[:, h * HD : (h + 1) * HD] = normed[
            h * seq_count : (h + 1) * seq_count
        ].astype(jnp.bfloat16)


def near(array):
    return pltpu.with_memory_space_constraint(array, pltpu.VMEM)


def local(
    prompt, forget_weight, value_weight, lower_bound, extra_decay, new_token, new_query, read_gain
):
    seq_count, span_len, width = prompt.shape
    width_dev = forget_weight.shape[1]
    head_count = width_dev // HD
    blocks = lax.axis_size("sp")
    peers = lax.axis_size("tp")
    row_share = HD // blocks
    groups = head_count * seq_count
    rows = HD // (blocks // groups) + 8
    anywhere = pl.BlockSpec(memory_space=pltpu.HBM)
    vmem = pl.BlockSpec(memory_space=pltpu.VMEM)
    lower_row = lower_bound[None]
    pair = lax.ppermute(new_token, "tp", [(i, i ^ 1) for i in range(peers)])
    sent = pl.pallas_call(
        dense_kernel,
        out_shape=pltpu.VMEM((blocks, rows, HD), jnp.float32),
        in_specs=[anywhere] * 5,
        out_specs=vmem,
        scratch_shapes=[
            pltpu.VMEM((seq_count, span_len, width), jnp.bfloat16),
            pltpu.VMEM((width, width_dev), jnp.bfloat16),
            pltpu.VMEM((width, width_dev), jnp.bfloat16),
            pltpu.VMEM((seq_count, span_len, width_dev), jnp.float32),
            pltpu.VMEM((1, width_dev), jnp.float32),
            pltpu.VMEM((groups, HD), jnp.float32),
            pltpu.SemaphoreType.DMA((3 * PIECES + 2 * (seq_count - 1) + 2,)),
        ],
        name="dense",
    )(prompt, forget_weight, value_weight, lower_row, extra_decay)
    sent = sent.astype(jnp.float16)
    got = lax.all_to_all(sent, "sp", 0, 0, tiled=True)
    token, pair, _ = lax.optimization_barrier((new_token, pair, sent))
    both = jnp.stack([token, pair])
    far = []
    for step in range(1, peers // 2):
        far.append(lax.ppermute(both, "tp", [(i, (i + 2 * step) % peers) for i in range(peers)]))
    others = len(far)
    part = width // (others + 1)
    sums, forget_far = pl.pallas_call(
        functools.partial(token_start_kernel, axis="tp"),
        out_shape=[
            pltpu.VMEM((2, seq_count, width_dev), jnp.float32),
            pltpu.VMEM((others, part, width_dev), jnp.bfloat16),
        ],
        in_specs=[vmem, vmem, anywhere, anywhere],
        out_specs=[vmem] * 2,
        scratch_shapes=[
            pltpu.VMEM((part, width_dev), jnp.bfloat16),
            pltpu.VMEM((part, width_dev), jnp.bfloat16),
            pltpu.SemaphoreType.DMA((others + 2,)),
        ],
        name="prepare",
    )(near(token), near(pair), forget_weight, value_weight)
    reach, addend = pl.pallas_call(
        functools.partial(token_kernel, axis="tp"),
        out_shape=[pltpu.VMEM((groups, HD), jnp.float32)] * 2,
        in_specs=[vmem] * (others + 2) + [anywhere, vmem, vmem],
        out_specs=[vmem] * 2,
        scratch_shapes=[
            pltpu.VMEM((others, part, width_dev), jnp.bfloat16),
            pltpu.SemaphoreType.DMA((others,)),
        ],
        name="token",
    )(
        *map(near, far), near(sums), near(forget_far), value_weight, near(lower_row),
        near(new_query),
    )
    got = near(got.astype(jnp.float32))
    shares = pl.pallas_call(
        functools.partial(state_kernel, axis="sp"),
        out_shape=pltpu.VMEM((blocks, row_share, HD), jnp.float32),
        in_specs=[vmem, vmem],
        out_specs=vmem,
        scratch_shapes=[
            pltpu.VMEM((HD, HD), jnp.float32),
            pltpu.VMEM((blocks, HD), jnp.float32),
        ],
        name="state",
    )(got, near(reach))
    shares = near(lax.all_to_all(shares, "sp", 0, 0, tiled=True))
    state_cache, first_read = pl.pallas_call(
        read_kernel,
        out_shape=[
            jax.ShapeDtypeStruct((row_share, head_count, seq_count, HD), jnp.bfloat16),
            jax.ShapeDtypeStruct((seq_count, width_dev), jnp.bfloat16),
        ],
        in_specs=[vmem] * 3,
        out_specs=[vmem] * 2,
        scratch_shapes=[pltpu.VMEM((blocks // groups + 1, row_share * groups, HD), jnp.float32)],
        name="read",
    )(shares, near(addend), near(read_gain[None]))
    return (state_cache, first_read)


def solution(mesh):
    return jax.shard_map(
        local,
        mesh=mesh,
        in_specs=(
            P(None, "sp", None),
            P(None, "tp"),
            P(None, "tp"),
            P("tp"),
            P(None, "sp", "tp"),
            P(None, "tp"),
            P(None, "tp"),
            P(),
        ),
        out_specs=(P("sp", "tp", None, None), P(None, "tp")),
        check_vma=False,
    )
```
